256 devices in a mesh: kv: 32 (over z, y), tp: 8 (over x, core).
Axes of the slice: x: 4, y: 4, z: 8, core: 2. Of those that a mesh axis runs over, the one named last changes fastest.
Arguments:
- residual_in: bfloat16 [256, 2048], P(None, ('kv', 'tp')), may hold values from -14 to 14
- delta_state: float32 [256, 32, 128, 128], P('kv', 'tp'), may hold values from -1 to 1
- norm_gain_first: float32 [2048], P('kv'), may hold values from 0.1 to 1.9
- gate_first: bfloat16 [2048, 5632], P('kv', 'tp'), may hold values from -0.125 to 0.125
- up_first: bfloat16 [2048, 5632], P('kv', 'tp'), may hold values from -0.125 to 0.125
- down_first: bfloat16 [5632, 2048], P('tp', 'kv'), may hold values from -0.15625 to 0.15625
- norm_gain_mixer: float32 [2048], P('kv'), may hold values from 0.1 to 1.9
- query_weight: bfloat16 [2048, 2048], P('kv', 'tp'), may hold values from -0.125 to 0.125
- key_weight: bfloat16 [2048, 2048], P('kv', 'tp'), may hold values from -0.125 to 0.125
- value_weight: bfloat16 [2048, 4096], P('kv', 'tp'), may hold values from -0.125 to 0.125
- output_gate_weight: bfloat16 [2048, 4096], P('kv', 'tp'), may hold values from -0.125 to 0.125
- beta_weight: bfloat16 [2048, 32], P('kv'), may hold values from -0.125 to 0.125
- decay_weight: bfloat16 [2048, 32], P('kv'), may hold values from -0.125 to 0.125
- decay_rate: float32 [32], P('tp'), may hold values from -2.3 to 1.1
- decay_bias: float32 [32], P('tp'), may hold values from -1 to 1
- head_gain: float32 [128], replicated, may hold values from 0.1 to 1.9
- out_weight: bfloat16 [4096, 2048], P('tp', 'kv'), may hold values from -0.125 to 0.125
- norm_gain_second: float32 [2048], P('kv'), may hold values from 0.1 to 1.9
- gate_second: bfloat16 [2048, 5632], P('kv', 'tp'), may hold values from -0.125 to 0.125
- up_second: bfloat16 [2048, 5632], P('kv', 'tp'), may hold values from -0.125 to 0.125
- down_second: bfloat16 [5632, 2048], P('tp', 'kv'), may hold values from -0.15625 to 0.15625
Outputs:
- residual_out: bfloat16 [256, 2048], P(None, ('kv', 'tp'))
- delta_state_out: float32 [256, 32, 128, 128], P('kv', 'tp')
The draws below stay inside these ranges and needn't reach their ends.
All inputs are finite; a program needn't handle non-finite values.
Results may differ from the reference program's by a relative error of at most 0.03.
Values may be sent and summed in bfloat16 or wider, within the bound.
No kernel may reach another device: no remote copies, remote signals or barrier semaphores. Data moves between devices by JAX's collectives and lax.ppermute only.
A program may use at most 64 MiB of HBM per device.

```python
import jax
import jax.numpy as jnp
from jax import lax

D = 2048
FF = 5632
K_HEADS = 16
HEAD = 128
V_HEADS = 32
KW = 2048
VW = 4096
BATCH = 256
N_TP = 8


def draw_residual_in(key, part):
    keys = jax.random.split(key, 4)
    region = jnp.arange(D, dtype=jnp.int32) // (D // 8)
    region_scale = jnp.exp(jax.random.uniform(keys[0], (8,), jnp.float32, -0.6, 0.6))
    column_scale = region_scale[region] * jnp.exp(jax.random.uniform(keys[1], (D,), jnp.float32, -0.2, 0.2))
    base = jnp.clip(jax.random.normal(keys[2], (BATCH, D), jnp.float32), -4.0, 4.0)
    row_scale = jnp.exp(jax.random.uniform(keys[3], (BATCH, 1), jnp.float32, -0.4, 0.4))
    return (base * row_scale * column_scale[None, :]).astype(jnp.bfloat16)


def shard_levels(own_key, dims, cuts, smallest, largest):
    loudness, own = 1.0, jax.random.fold_in(own_key, 6)
    for dim, shards_of in cuts:
        draws = jnp.exp(jax.random.uniform(jax.random.fold_in(own, dim), (shards_of,), jnp.float32, smallest / len(cuts), largest / len(cuts)))
        loudness = loudness * jnp.repeat(draws, dims[dim] // shards_of).reshape([-1 if axis == dim else 1 for axis in range(len(dims))])
    return loudness


def bell_draw(rng, dims, spread, reach, cuts=(), kind=jnp.bfloat16):
    factor_of = shard_levels(rng, dims, cuts, -0.22, 0.18) if cuts else 1.0
    result = jax.random.normal(rng, dims, jnp.float32) * spread * factor_of
    return jnp.minimum(jnp.maximum(result, -reach), reach).astype(kind)


def setup_inputs(seed: int = 0) -> dict:
    key_list = jax.random.split(jax.random.key(seed), 22)
    return {
        "residual_in": draw_residual_in(jax.random.fold_in(key_list[21], 71), 0),
        "delta_state": bell_draw(key_list[1], (BATCH, V_HEADS, HEAD, HEAD), 0.2, 1.0, ((0, 32), (1, 8)), jnp.float32),
        "norm_gain_first": jnp.clip(1.0 + 0.18 * jax.random.normal(key_list[2], (D,), jnp.float32), 0.1, 1.9),
        "gate_first": bell_draw(key_list[3], (D, FF), D ** -0.5, 0.125, ((0, 32), (1, 8))),
        "up_first": bell_draw(key_list[4], (D, FF), D ** -0.5, 0.125, ((0, 32), (1, 8))),
        "down_first": bell_draw(key_list[5], (FF, D), (FF // 4) ** -0.5, 0.15625, ((0, 8), (1, 32))),
        "norm_gain_mixer": jnp.clip(1.0 + 0.18 * jax.random.normal(key_list[6], (D,), jnp.float32), 0.1, 1.9),
        "query_weight": bell_draw(key_list[7], (D, KW), D ** -0.5, 0.125, ((0, 32), (1, 8))),
        "key_weight": bell_draw(key_list[8], (D, KW), D ** -0.5, 0.125, ((0, 32), (1, 8))),
        "value_weight": bell_draw(key_list[9], (D, VW), D ** -0.5, 0.125, ((0, 32), (1, 8))),
        "output_gate_weight": bell_draw(key_list[10], (D, VW), D ** -0.5, 0.125, ((0, 32), (1, 8))),
        "beta_weight": bell_draw(key_list[11], (D, V_HEADS), D ** -0.5, 0.125, ((0, 32),)),
        "decay_weight": bell_draw(key_list[12], (D, V_HEADS), D ** -0.5, 0.125, ((0, 32),)),
        "decay_rate": jnp.clip(-2.3 + 3.4 * jax.random.uniform(key_list[13], (V_HEADS,), jnp.float32) ** shard_levels(key_list[13], (V_HEADS,), ((0, 8),), -0.2, 0.2), -2.3, 1.1),
        "decay_bias": jnp.clip(jax.random.uniform(key_list[14], (V_HEADS,), jnp.float32, -1.0, 1.0) * shard_levels(key_list[14], (V_HEADS,), ((0, 8),), -0.4, 0.0), -1.0, 1.0),
        "head_gain": jnp.clip(1.0 + 0.18 * jax.random.normal(key_list[15], (HEAD,), jnp.float32), 0.1, 1.9),
        "out_weight": bell_draw(key_list[16], (VW, D), (VW // 2) ** -0.5, 0.125, ((0, 8), (1, 32))),
        "norm_gain_second": jnp.clip(1.0 + 0.18 * jax.random.normal(key_list[17], (D,), jnp.float32), 0.1, 1.9),
        "gate_second": bell_draw(key_list[18], (D, FF), D ** -0.5, 0.125, ((0, 32), (1, 8))),
        "up_second": bell_draw(key_list[19], (D, FF), D ** -0.5, 0.125, ((0, 32), (1, 8))),
        "down_second": bell_draw(key_list[20], (FF, D), (FF // 4) ** -0.5, 0.15625, ((0, 8), (1, 32))),
    }


epsilon = 1e-06

def head_sums(left_side, right_side):
    left_parts = left_side.reshape(left_side.shape[0], N_TP, -1).astype(jnp.float32)
    weights = right_side.reshape(N_TP, -1, right_side.shape[1]).astype(jnp.float32)
    pieces = jnp.einsum('btf,tfd->tbd', left_parts, weights)
    rounded = lax.optimization_barrier(pieces.astype(jnp.bfloat16))
    return lax.optimization_barrier(jnp.sum(rounded.astype(jnp.float32), axis=0))

def norm_parts(residual, norm_gain):
    as_float = residual.astype(jnp.float32)
    rowscale = lax.rsqrt(lax.optimization_barrier(jnp.sum(as_float * as_float, axis=1, keepdims=True)) / D + epsilon)
    scaled = (as_float * norm_gain).astype(jnp.bfloat16)
    return (as_float, rowscale, scaled)

def half_ffn(residual, norm_gain, gate_weight, up_weight, down_weight):
    as_float, rowscale, scaled = norm_parts(residual, norm_gain)
    gate_act = jnp.dot(scaled, gate_weight, preferred_element_type=jnp.float32) * rowscale
    up_act = jnp.dot(scaled, up_weight, preferred_element_type=jnp.float32) * rowscale
    hidden = (jax.nn.silu(gate_act) * up_act).astype(jnp.bfloat16)
    branch = head_sums(hidden, down_weight)
    return (as_float + 0.5 * branch).astype(jnp.bfloat16)

def unit_heads(projected, head_size):
    activated = jax.nn.silu(projected).reshape(projected.shape[0], -1, head_size)
    return activated * lax.rsqrt(lax.optimization_barrier(jnp.sum(activated * activated, axis=-1, keepdims=True)) + epsilon)

def delta_step(old_state, key_rows, queries, values, beta_gate, decay_gate):
    faded_state = old_state * decay_gate[:, :, None, None]
    predicted = jnp.einsum('rhab,rha->rhb', faded_state, key_rows, precision=lax.Precision.HIGHEST)
    correction = beta_gate[:, :, None] * (values - predicted)
    updated = faded_state + key_rows[:, :, :, None] * correction[:, :, None, :]
    reading = jnp.einsum('rhab,rha->rhb', updated, queries, precision=lax.Precision.HIGHEST)
    return (updated, reading)

def advance(inputs):
    return delta_step(*inputs)

def reference(residual_in, delta_state, norm_gain_first, gate_first, up_first, down_first, norm_gain_mixer, query_weight, key_weight, value_weight, output_gate_weight, beta_weight, decay_weight, decay_rate, decay_bias, head_gain, out_weight, norm_gain_second, gate_second, up_second, down_second):
    after_first = half_ffn(residual_in, norm_gain_first, gate_first, up_first, down_first)
    as_float, rowscale, scaled = norm_parts(after_first, norm_gain_mixer)

    def project(weight):
        return jnp.dot(scaled, weight, preferred_element_type=jnp.float32) * rowscale
    repeat_count = V_HEADS // K_HEADS
    queries = jnp.repeat(unit_heads(project(query_weight), HEAD) * HEAD ** (-0.5), repeat_count, axis=1)
    key_rows = jnp.repeat(unit_heads(project(key_weight), HEAD), repeat_count, axis=1)
    values = jax.nn.silu(project(value_weight)).reshape(BATCH, V_HEADS, HEAD)
    out_gate = jax.nn.silu(project(output_gate_weight)).reshape(BATCH, V_HEADS, HEAD)
    beta_gate = jax.nn.sigmoid(project(beta_weight))
    decay_gate = jnp.exp(-jnp.exp(decay_rate)[None, :] * jax.nn.softplus(project(decay_weight) + decay_bias[None, :]))
    groups = BATCH // 8
    stacked = tuple((item.reshape((groups, BATCH // groups) + item.shape[1:]) for item in (delta_state, key_rows, queries, values, beta_gate, decay_gate)))
    new_state, reading = lax.map(advance, stacked)
    new_state = new_state.reshape(BATCH, V_HEADS, HEAD, HEAD)
    reading = reading.reshape(BATCH, V_HEADS, HEAD)
    normed = reading * lax.rsqrt(lax.optimization_barrier(jnp.mean(reading * reading, axis=-1, keepdims=True)) + epsilon)
    normed = (normed * head_gain * out_gate).reshape(BATCH, VW).astype(jnp.bfloat16)
    after_mixer = (as_float + head_sums(normed, out_weight)).astype(jnp.bfloat16)
    residual_out = half_ffn(after_mixer, norm_gain_second, gate_second, up_second, down_second)
    return (residual_out, new_state)
```

```python
import jax
import jax.numpy as jnp
from jax import lax
from jax.sharding import Mesh
from jax.sharding import PartitionSpec as P

D = 2048
HEAD = 128
GATES = 128

epsilon = 1e-06

TP = ("x", "c")
ACROSS = ("z", "x", "c")

bf16 = jnp.bfloat16
f32 = jnp.float32


def exchange(blocks, axis):
    return lax.all_to_all(blocks, axis, split_axis=0, concat_axis=0, tiled=True)


def from_everyone(value, axis):
    return exchange(jnp.broadcast_to(value, (lax.axis_size(axis), *value.shape)), axis)


def everyone_sum(value, axis):
    return from_everyone(value, axis).astype(f32).sum(axis=0)


def times_transposed(left, right_rows):
    return lax.dot_general(left, right_rows, (((1,), (1,)), ((), ())), preferred_element_type=f32)


def square_columns(as_float):
    squares = jnp.sum(as_float * as_float, axis=1, keepdims=True)
    high = squares.astype(bf16).astype(f32)
    lane = lax.broadcasted_iota(jnp.int32, (squares.shape[0], GATES), 1)
    return jnp.where(lane == 0, high, jnp.where(lane == 1, squares - high, 0.0))


def row_scale(first_two):
    return lax.rsqrt((first_two[:, :1] + first_two[:, 1:2]) / D + epsilon)


def hidden_units(residual, gate_up):
    partial_value = jnp.dot(residual, gate_up, preferred_element_type=f32)
    both = jnp.concatenate([partial_value, square_columns(residual.astype(f32))], axis=1).astype(bf16)
    summed = everyone_sum(both, "y")
    width = gate_up.shape[1]
    scale = row_scale(summed[:, width:])
    gate_act = summed[:, : width // 2] * scale
    up_act = summed[:, width // 2 : width] * scale
    return (jax.nn.silu(gate_act) * up_act).astype(bf16)


def unit_heads(projected, head_size):
    activated = jax.nn.silu(projected).reshape(projected.shape[0], -1, head_size)
    return activated * lax.rsqrt(jnp.sum(activated * activated, axis=-1, keepdims=True) + epsilon)


def delta_step(old_state, key_rows, queries, values, beta_gate, decay_gate):
    faded_state = old_state * decay_gate[:, :, None, None]
    predicted = jnp.einsum("rhab,rha->rhb", faded_state, key_rows, precision=lax.Precision.HIGHEST)
    correction = beta_gate[:, :, None] * (values - predicted)
    updated = faded_state + key_rows[:, :, :, None] * correction[:, :, None, :]
    reading = jnp.einsum("rhab,rha->rhb", updated, queries, precision=lax.Precision.HIGHEST)
    return (updated, reading)


def mixer_values(residual, mixer_in, decay_rate, decay_bias, head_gain, old_state):
    row_count, heads_dev, head_size = old_state.shape[:3]
    projected = jnp.dot(residual, mixer_in, preferred_element_type=f32)
    width = mixer_in.shape[1] - GATES
    squares = square_columns(residual.astype(f32))
    tail = projected[:, width:] + jnp.roll(squares, 2 * heads_dev, axis=1)
    both = jnp.concatenate([projected[:, :width], tail], axis=1).astype(bf16)
    blocks = both.reshape(-1, row_count, both.shape[1])
    summed = exchange(blocks, "y").astype(f32).sum(axis=0)
    tail = summed[:, width:]
    scale = row_scale(tail[:, 2 * heads_dev :])
    summed = summed[:, :width] * scale
    gates = tail * scale
    value_cols = heads_dev * head_size
    key_cols = (width - 2 * value_cols) // 2
    repeat_count = value_cols // key_cols
    queries = jnp.repeat(
        unit_heads(summed[:, :key_cols], head_size) * head_size ** (-0.5), repeat_count, axis=1
    )
    key_rows = jnp.repeat(unit_heads(summed[:, key_cols : 2 * key_cols], head_size), repeat_count, axis=1)
    values = jax.nn.silu(summed[:, 2 * key_cols : 2 * key_cols + value_cols]).reshape(
        row_count, heads_dev, head_size
    )
    out_gate = jax.nn.silu(summed[:, 2 * key_cols + value_cols :]).reshape(row_count, heads_dev, head_size)
    beta_gate = jax.nn.sigmoid(gates[:, :heads_dev])
    decay_gate = jnp.exp(
        -jnp.exp(decay_rate)[None, :]
        * jax.nn.softplus(gates[:, heads_dev : 2 * heads_dev] + decay_bias[None, :])
    )
    new_state, reading = delta_step(old_state, key_rows, queries, values, beta_gate, decay_gate)
    normed = reading * lax.rsqrt(jnp.mean(reading * reading, axis=-1, keepdims=True) + epsilon)
    normed = (normed * head_gain * out_gate).reshape(row_count, value_cols).astype(bf16)
    return normed, new_state


def body(
    residual_in,
    delta_state,
    norm_gain_first,
    gate_first,
    up_first,
    down_first,
    norm_gain_mixer,
    query_weight,
    key_weight,
    value_weight,
    output_gate_weight,
    beta_weight,
    decay_weight,
    decay_rate,
    decay_bias,
    head_gain,
    out_weight,
    norm_gain_second,
    gate_second,
    up_second,
    down_second,
):
    planes, tp_count = lax.axis_size("z"), lax.axis_size(TP)
    heads_dev = decay_rate.shape[0]

    def scaled_rows(gain, weights):
        return (jnp.concatenate(weights, axis=1).astype(f32) * gain[:, None]).astype(bf16)

    def gathered(weights):
        return lax.all_gather(jnp.concatenate(weights, axis=1), "z", axis=0, tiled=True)

    head_start = lax.axis_index(TP) * heads_dev
    gate_cols = [
        lax.dynamic_slice_in_dim(beta_weight, head_start, heads_dev, 1),
        lax.dynamic_slice_in_dim(decay_weight, head_start, heads_dev, 1),
        jnp.zeros((beta_weight.shape[0], GATES - 2 * heads_dev), bf16),
    ]
    first_in = scaled_rows(norm_gain_first, [gate_first, up_first])
    mixer_in = scaled_rows(
        norm_gain_mixer, [query_weight, key_weight, value_weight, output_gate_weight, *gate_cols]
    )
    second_in = scaled_rows(norm_gain_second, [gate_second, up_second])
    width, mixer_width = first_in.shape[1], mixer_in.shape[1]
    first_in = gathered([first_in])
    middle = gathered([down_first.T, mixer_in])
    last = gathered([out_weight.T, second_in, down_second.T])
    down_first, mixer_in = middle[:, : width // 2], middle[:, width // 2 :]
    values_width = out_weight.shape[0]
    out_rows, second_in, down_second = (
        last[:, :values_width],
        last[:, values_width : values_width + width],
        last[:, values_width + width :],
    )

    columns = residual_in.T
    own_cols, rows = columns.shape[0], columns.shape[1] // planes
    pieces = jnp.moveaxis(columns.reshape(own_cols, planes, rows), 1, 0)
    pieces = jnp.broadcast_to(pieces[:, None], (planes, tp_count, own_cols, rows))
    residual = exchange(pieces.reshape(-1, own_cols, rows), ACROSS).reshape(-1, rows).T

    hidden = hidden_units(residual, first_in)
    projected = times_transposed(hidden, down_first).astype(bf16)
    after_first = (residual.astype(f32) + 0.5 * everyone_sum(projected, TP)).astype(bf16)

    normed, new_state = mixer_values(
        after_first, mixer_in, decay_rate, decay_bias, head_gain, delta_state
    )
    normed = from_everyone(normed, "y").reshape(rows, -1)
    projected = times_transposed(normed, out_rows).astype(bf16)
    after_mixer = (after_first.astype(f32) + everyone_sum(projected, TP)).astype(bf16)

    hidden = hidden_units(after_mixer, second_in)
    projected = times_transposed(down_second, hidden).astype(bf16)
    pieces = jnp.concatenate([projected, after_mixer.T], axis=1)
    arrived = exchange(pieces.reshape(-1, own_cols, 2 * rows), ACROSS)
    arrived = arrived.reshape(planes, tp_count, own_cols, 2 * rows).astype(f32)
    final = arrived[:, 0, :, rows:] + 0.5 * arrived[..., :rows].sum(axis=1)
    residual_out = jnp.moveaxis(final, 1, 2).reshape(planes * rows, own_cols).astype(bf16)
    return (residual_out, new_state)


def solution(mesh):
    cut = Mesh(mesh.devices.reshape(8, 4, 4, 2), ("z", "y", "x", "c"))
    kv, tp = ("z", "y"), ("x", "c")
    wide, tall = P(kv, tp), P(tp, kv)
    placed = (
        P(None, kv + tp),
        P(kv, tp, None, None),
        P(kv),
        wide,
        wide,
        tall,
        P(kv),
        wide,
        wide,
        wide,
        wide,
        P(kv, None),
        P(kv, None),
        P(tp),
        P(tp),
        P(),
        tall,
        P(kv),
        wide,
        wide,
        tall,
    )
    return jax.shard_map(
        body,
        mesh=cut,
        in_specs=placed,
        out_specs=(P(None, kv + tp), P(kv, tp, None, None)),
        check_vma=False,
    )
```

```python
import jax
import jax.numpy as jnp
from jax import lax
from jax.sharding import Mesh
from jax.sharding import PartitionSpec as P

D = 2048
HEAD = 128
GATES = 128

epsilon = 1e-06

TP = ("x", "c")
ACROSS = ("z", "x", "c")

bf16 = jnp.bfloat16
f32 = jnp.float32


def exchange(blocks, axis):
    return lax.all_to_all(blocks, axis, split_axis=0, concat_axis=0, tiled=True)


def from_everyone(value, axis):
    return exchange(jnp.broadcast_to(value, (lax.axis_size(axis), *value.shape)), axis)


def everyone_sum(value, axis):
    return from_everyone(value, axis).astype(f32).sum(axis=0)


def times_transposed(left, right_rows):
    return lax.dot_general(left, right_rows, (((1,), (1,)), ((), ())), preferred_element_type=f32)


def square_columns(as_float):
    squares = jnp.sum(as_float * as_float, axis=1, keepdims=True)
    high = squares.astype(bf16).astype(f32)
    lane = lax.broadcasted_iota(jnp.int32, (squares.shape[0], GATES), 1)
    return jnp.where(lane == 0, high, jnp.where(lane == 1, squares - high, 0.0))


def row_scale(first_two):
    return lax.rsqrt((first_two[:, :1] + first_two[:, 1:2]) / D + epsilon)


def around(block, axis):
    size = lax.axis_size(axis)
    ahead = [(i, (i + 1) % size) for i in range(size)]
    behind = [(i, (i - 1) % size) for i in range(size)]
    blocks = [block] + [None] * (size - 1)
    forward = backward = block
    for step in range(1, size // 2):
        forward = blocks[size - step] = lax.ppermute(forward, axis, ahead)
        backward = blocks[step] = lax.ppermute(backward, axis, behind)
    half = block.shape[1] // 2
    forward = lax.ppermute(forward[:, :half], axis, ahead)
    backward = lax.ppermute(backward[:, half:], axis, behind)
    blocks[size // 2] = jnp.concatenate([forward, backward], axis=1)
    return blocks


def hidden_units(residual, partial_value):
    both = jnp.concatenate([partial_value, square_columns(residual.astype(f32))], axis=1).astype(bf16)
    summed = everyone_sum(both, "y")
    width = partial_value.shape[1]
    scale = row_scale(summed[:, width:])
    gate_act = summed[:, : width // 2] * scale
    up_act = summed[:, width // 2 : width] * scale
    return (jax.nn.silu(gate_act) * up_act).astype(bf16)


def unit_heads(projected, head_size):
    activated = jax.nn.silu(projected).reshape(projected.shape[0], -1, head_size)
    return activated * lax.rsqrt(jnp.sum(activated * activated, axis=-1, keepdims=True) + epsilon)


def delta_step(old_state, key_rows, queries, values, beta_gate, decay_gate):
    faded_state = old_state * decay_gate[:, :, None, None]
    predicted = jnp.einsum("rhab,rha->rhb", faded_state, key_rows, precision=lax.Precision.HIGHEST)
    correction = beta_gate[:, :, None] * (values - predicted)
    updated = faded_state + key_rows[:, :, :, None] * correction[:, :, None, :]
    reading = jnp.einsum("rhab,rha->rhb", updated, queries, precision=lax.Precision.HIGHEST)
    return (updated, reading)


def mixer_values(residual, mixer_in, decay_rate, decay_bias, head_gain, old_state):
    row_count, heads_dev, head_size = old_state.shape[:3]
    projected = jnp.dot(residual, mixer_in, preferred_element_type=f32)
    width = mixer_in.shape[1] - GATES
    squares = square_columns(residual.astype(f32))
    tail = projected[:, width:] + jnp.roll(squares, 2 * heads_dev, axis=1)
    both = jnp.concatenate([projected[:, :width], tail], axis=1).astype(bf16)
    blocks = both.reshape(-1, row_count, both.shape[1])
    summed = exchange(blocks, "y").astype(f32).sum(axis=0)
    tail = summed[:, width:]
    scale = row_scale(tail[:, 2 * heads_dev :])
    summed = summed[:, :width] * scale
    gates = tail * scale
    value_cols = heads_dev * head_size
    key_cols = (width - 2 * value_cols) // 2
    repeat_count = value_cols // key_cols
    queries = jnp.repeat(
        unit_heads(summed[:, :key_cols], head_size) * head_size ** (-0.5), repeat_count, axis=1
    )
    key_rows = jnp.repeat(unit_heads(summed[:, key_cols : 2 * key_cols], head_size), repeat_count, axis=1)
    values = jax.nn.silu(summed[:, 2 * key_cols : 2 * key_cols + value_cols]).reshape(
        row_count, heads_dev, head_size
    )
    out_gate = jax.nn.silu(summed[:, 2 * key_cols + value_cols :]).reshape(row_count, heads_dev, head_size)
    beta_gate = jax.nn.sigmoid(gates[:, :heads_dev])
    decay_gate = jnp.exp(
        -jnp.exp(decay_rate)[None, :]
        * jax.nn.softplus(gates[:, heads_dev : 2 * heads_dev] + decay_bias[None, :])
    )
    new_state, reading = delta_step(old_state, key_rows, queries, values, beta_gate, decay_gate)
    normed = reading * lax.rsqrt(jnp.mean(reading * reading, axis=-1, keepdims=True) + epsilon)
    normed = (normed * head_gain * out_gate).reshape(row_count, value_cols).astype(bf16)
    return normed, new_state


def body(
    residual_in,
    delta_state,
    norm_gain_first,
    gate_first,
    up_first,
    down_first,
    norm_gain_mixer,
    query_weight,
    key_weight,
    value_weight,
    output_gate_weight,
    beta_weight,
    decay_weight,
    decay_rate,
    decay_bias,
    head_gain,
    out_weight,
    norm_gain_second,
    gate_second,
    up_second,
    down_second,
):
    planes, tp_count = lax.axis_size("z"), lax.axis_size(TP)
    heads_dev = decay_rate.shape[0]

    def scaled_rows(gain, weights):
        return (jnp.concatenate(weights, axis=1).astype(f32) * gain[:, None]).astype(bf16)

    def gathered(weights):
        return lax.all_gather(jnp.concatenate(weights, axis=1), "z", axis=0, tiled=True)

    head_start = lax.axis_index(TP) * heads_dev
    gate_cols = [
        lax.dynamic_slice_in_dim(beta_weight, head_start, heads_dev, 1),
        lax.dynamic_slice_in_dim(decay_weight, head_start, heads_dev, 1),
        jnp.zeros((beta_weight.shape[0], GATES - 2 * heads_dev), bf16),
    ]
    first_in = scaled_rows(norm_gain_first, [gate_first, up_first])
    mixer_in = scaled_rows(
        norm_gain_mixer, [query_weight, key_weight, value_weight, output_gate_weight, *gate_cols]
    )
    second_in = scaled_rows(norm_gain_second, [gate_second, up_second])
    width, mixer_width = first_in.shape[1], mixer_in.shape[1]
    first_blocks = around(first_in, "z")
    middle = gathered([down_first.T, mixer_in])
    last = gathered([out_weight.T, second_in, down_second.T])
    down_first, mixer_in = middle[:, : width // 2], middle[:, width // 2 :]
    values_width = out_weight.shape[0]
    out_rows, second_in, down_second = (
        last[:, :values_width],
        last[:, values_width : values_width + width],
        last[:, values_width + width :],
    )

    columns = residual_in.T
    own_cols, rows = columns.shape[0], columns.shape[1] // planes
    pieces = jnp.moveaxis(columns.reshape(own_cols, planes, rows), 1, 0)
    pieces = jnp.broadcast_to(pieces[:, None], (planes, tp_count, own_cols, rows))
    arrived = exchange(pieces.reshape(-1, own_cols, rows), ACROSS).reshape(planes, -1, rows)
    residual = arrived.reshape(-1, rows).T
    twice = jnp.concatenate([arrived, arrived], axis=0)
    ahead = lax.dynamic_slice_in_dim(twice, lax.axis_index("z"), planes, 0)
    products = [
        lax.dot_general(ahead[o], first_blocks[o], (((0,), (0,)), ((), ())), preferred_element_type=f32)
        for step in range(planes // 2 + 1)
        for o in sorted({step, (planes - step) % planes})
    ]
    partial_value = products[0]
    for product in products[1:]:
        partial_value = partial_value + product

    hidden = hidden_units(residual, partial_value)
    projected = times_transposed(hidden, down_first).astype(bf16)
    after_first = (residual.astype(f32) + 0.5 * everyone_sum(projected, TP)).astype(bf16)

    normed, new_state = mixer_values(
        after_first, mixer_in, decay_rate, decay_bias, head_gain, delta_state
    )
    normed = from_everyone(normed, "y").reshape(rows, -1)
    projected = times_transposed(normed, out_rows).astype(bf16)
    after_mixer = (after_first.astype(f32) + everyone_sum(projected, TP)).astype(bf16)

    hidden = hidden_units(after_mixer, jnp.dot(after_mixer, second_in, preferred_element_type=f32))
    projected = times_transposed(down_second, hidden).astype(bf16)
    pieces = jnp.concatenate([projected, after_mixer.T], axis=1)
    arrived = exchange(pieces.reshape(-1, own_cols, 2 * rows), ACROSS)
    arrived = arrived.reshape(planes, tp_count, own_cols, 2 * rows).astype(f32)
    final = arrived[:, 0, :, rows:] + 0.5 * arrived[..., :rows].sum(axis=1)
    residual_out = jnp.moveaxis(final, 1, 2).reshape(planes * rows, own_cols).astype(bf16)
    return (residual_out, new_state)


def solution(mesh):
    cut = Mesh(mesh.devices.reshape(8, 4, 4, 2), ("z", "y", "x", "c"))
    kv, tp = ("z", "y"), ("x", "c")
    wide, tall = P(kv, tp), P(tp, kv)
    placed = (
        P(None, kv + tp),
        P(kv, tp, None, None),
        P(kv),
        wide,
        wide,
        tall,
        P(kv),
        wide,
        wide,
        wide,
        wide,
        P(kv, None),
        P(kv, None),
        P(tp),
        P(tp),
        P(),
        tall,
        P(kv),
        wide,
        wide,
        tall,
    )
    return jax.shard_map(
        body,
        mesh=cut,
        in_specs=placed,
        out_specs=(P(None, kv + tp), P(kv, tp, None, None)),
        check_vma=False,
    )
```

```python
import jax
import jax.numpy as jnp
from jax import lax
from jax.sharding import Mesh
from jax.sharding import PartitionSpec as P

D = 2048
HEAD = 128
GATES = 128

epsilon = 1e-06

TP = ("x", "c")
ACROSS = ("z", "x", "c")

bf16 = jnp.bfloat16
f32 = jnp.float32


def exchange(blocks, axis):
    return lax.all_to_all(blocks, axis, split_axis=0, concat_axis=0, tiled=True)


def from_everyone(value, axis):
    return exchange(jnp.broadcast_to(value, (lax.axis_size(axis), *value.shape)), axis)


def everyone_sum(value, axis):
    return from_everyone(value, axis).astype(f32).sum(axis=0)


def ring_sum(value, axis):
    size = lax.axis_size(axis)
    total = value.astype(f32)
    for places in range(1, size):
        total = total + lax.ppermute(value, axis, [(i, (i + places) % size) for i in range(size)]).astype(f32)
    return total


def times_transposed(left, right_rows):
    return lax.dot_general(left, right_rows, (((1,), (1,)), ((), ())), preferred_element_type=f32)


def square_columns(as_float):
    squares = jnp.sum(as_float * as_float, axis=1, keepdims=True)
    high = squares.astype(bf16).astype(f32)
    lane = lax.broadcasted_iota(jnp.int32, (squares.shape[0], GATES), 1)
    return jnp.where(lane == 0, high, jnp.where(lane == 1, squares - high, 0.0))


def row_scale(first_two):
    return lax.rsqrt((first_two[:, :1] + first_two[:, 1:2]) / D + epsilon)


def around(block, axis):
    size = lax.axis_size(axis)
    ahead = [(i, (i + 1) % size) for i in range(size)]
    behind = [(i, (i - 1) % size) for i in range(size)]
    blocks = [block] + [None] * (size - 1)
    forward = backward = block
    for step in range(1, size // 2):
        forward = blocks[size - step] = lax.ppermute(forward, axis, ahead)
        backward = blocks[step] = lax.ppermute(backward, axis, behind)
    half = block.shape[1] // 2
    forward = lax.ppermute(forward[:, :half], axis, ahead)
    backward = lax.ppermute(backward[:, half:], axis, behind)
    blocks[size // 2] = jnp.concatenate([forward, backward], axis=1)
    return blocks


def hidden_units(residual, partial_value):
    both = jnp.concatenate([partial_value, square_columns(residual.astype(f32))], axis=1).astype(bf16)
    summed = ring_sum(both, "y")
    width = partial_value.shape[1]
    scale = row_scale(summed[:, width:])
    gate_act = summed[:, : width // 2] * scale
    up_act = summed[:, width // 2 : width] * scale
    return (jax.nn.silu(gate_act) * up_act).astype(bf16)


def unit_heads(projected, head_size):
    activated = jax.nn.silu(projected).reshape(projected.shape[0], -1, head_size)
    return activated * lax.rsqrt(jnp.sum(activated * activated, axis=-1, keepdims=True) + epsilon)


def delta_step(old_state, key_rows, queries, values, beta_gate, decay_gate):
    faded_state = old_state * decay_gate[:, :, None, None]
    predicted = jnp.einsum("rhab,rha->rhb", faded_state, key_rows, precision=lax.Precision.HIGHEST)
    correction = beta_gate[:, :, None] * (values - predicted)
    updated = faded_state + key_rows[:, :, :, None] * correction[:, :, None, :]
    reading = jnp.einsum("rhab,rha->rhb", updated, queries, precision=lax.Precision.HIGHEST)
    return (updated, reading)


def mixer_values(residual, mixer_in, decay_rate, decay_bias, head_gain, old_state):
    row_count, heads_dev, head_size = old_state.shape[:3]
    projected = jnp.dot(residual, mixer_in, preferred_element_type=f32)
    width = mixer_in.shape[1] - GATES
    squares = square_columns(residual.astype(f32))
    tail = projected[:, width:] + jnp.roll(squares, 2 * heads_dev, axis=1)
    both = jnp.concatenate([projected[:, :width], tail], axis=1).astype(bf16)
    blocks = both.reshape(-1, row_count, both.shape[1])
    summed = exchange(blocks, "y").astype(f32).sum(axis=0)
    tail = summed[:, width:]
    scale = row_scale(tail[:, 2 * heads_dev :])
    summed = summed[:, :width] * scale
    gates = tail * scale
    value_cols = heads_dev * head_size
    key_cols = (width - 2 * value_cols) // 2
    repeat_count = value_cols // key_cols
    queries = jnp.repeat(
        unit_heads(summed[:, :key_cols], head_size) * head_size ** (-0.5), repeat_count, axis=1
    )
    key_rows = jnp.repeat(unit_heads(summed[:, key_cols : 2 * key_cols], head_size), repeat_count, axis=1)
    values = jax.nn.silu(summed[:, 2 * key_cols : 2 * key_cols + value_cols]).reshape(
        row_count, heads_dev, head_size
    )
    out_gate = jax.nn.silu(summed[:, 2 * key_cols + value_cols :]).reshape(row_count, heads_dev, head_size)
    beta_gate = jax.nn.sigmoid(gates[:, :heads_dev])
    decay_gate = jnp.exp(
        -jnp.exp(decay_rate)[None, :]
        * jax.nn.softplus(gates[:, heads_dev : 2 * heads_dev] + decay_bias[None, :])
    )
    new_state, reading = delta_step(old_state, key_rows, queries, values, beta_gate, decay_gate)
    normed = reading * lax.rsqrt(jnp.mean(reading * reading, axis=-1, keepdims=True) + epsilon)
    normed = (normed * head_gain * out_gate).reshape(row_count, value_cols).astype(bf16)
    return normed, new_state


def body(
    residual_in,
    delta_state,
    norm_gain_first,
    gate_first,
    up_first,
    down_first,
    norm_gain_mixer,
    query_weight,
    key_weight,
    value_weight,
    output_gate_weight,
    beta_weight,
    decay_weight,
    decay_rate,
    decay_bias,
    head_gain,
    out_weight,
    norm_gain_second,
    gate_second,
    up_second,
    down_second,
):
    planes, tp_count = lax.axis_size("z"), lax.axis_size(TP)
    heads_dev = decay_rate.shape[0]

    def scaled_rows(gain, weights):
        return (jnp.concatenate(weights, axis=1).astype(f32) * gain[:, None]).astype(bf16)

    def gathered(weights):
        return lax.all_gather(jnp.concatenate(weights, axis=1), "z", axis=0, tiled=True)

    head_start = lax.axis_index(TP) * heads_dev
    gate_cols = [
        lax.dynamic_slice_in_dim(beta_weight, head_start, heads_dev, 1),
        lax.dynamic_slice_in_dim(decay_weight, head_start, heads_dev, 1),
        jnp.zeros((beta_weight.shape[0], GATES - 2 * heads_dev), bf16),
    ]
    first_in = scaled_rows(norm_gain_first, [gate_first, up_first])
    first_in, query_weight, gate_cols[0], gate_cols[1], down_first = lax.optimization_barrier(
        (first_in, query_weight, gate_cols[0], gate_cols[1], down_first)
    )
    mixer_in = scaled_rows(
        norm_gain_mixer, [query_weight, key_weight, value_weight, output_gate_weight, *gate_cols]
    )
    second_in = scaled_rows(norm_gain_second, [gate_second, up_second])
    width, mixer_width = first_in.shape[1], mixer_in.shape[1]
    first_blocks = around(first_in, "z")
    middle = jnp.concatenate([mixer_in, down_first.T], axis=1)
    middle, residual_in = lax.optimization_barrier((middle, residual_in))
    middle = gathered([middle])
    mixer_in, down_first = middle[:, :mixer_width], middle[:, mixer_width:]
    last = jnp.concatenate([out_weight.T, second_in, down_second.T], axis=1)
    first_blocks[3], last = lax.optimization_barrier((first_blocks[3], last))
    last = gathered([last])
    values_width = out_weight.shape[0]
    out_rows, second_in, down_second = (
        last[:, :values_width],
        last[:, values_width : values_width + width],
        last[:, values_width + width :],
    )

    columns = residual_in.T
    own_cols, rows = columns.shape[0], columns.shape[1] // planes
    pieces = jnp.moveaxis(columns.reshape(own_cols, planes, rows), 1, 0)
    pieces = jnp.broadcast_to(pieces[:, None], (planes, tp_count, own_cols, rows))
    arrived = exchange(pieces.reshape(-1, own_cols, rows), ACROSS).reshape(planes, -1, rows)
    arrived, first_blocks[2], first_blocks[-2] = lax.optimization_barrier(
        (arrived, first_blocks[2], first_blocks[-2])
    )
    residual = arrived.reshape(-1, rows).T
    twice = jnp.concatenate([arrived, arrived], axis=0)
    ahead = lax.dynamic_slice_in_dim(twice, lax.axis_index("z"), planes, 0)
    products = [
        lax.dot_general(ahead[o], first_blocks[o], (((0,), (0,)), ((), ())), preferred_element_type=f32)
        for step in range(planes // 2 + 1)
        for o in sorted({step, (planes - step) % planes})
    ]
    partial_value = products[0]
    for product in products[1:]:
        partial_value = partial_value + product

    hidden = hidden_units(residual, partial_value)
    projected = times_transposed(hidden, down_first).astype(bf16)
    after_first = (residual.astype(f32) + 0.5 * everyone_sum(projected, TP)).astype(bf16)

    normed, new_state = mixer_values(
        after_first, mixer_in, decay_rate, decay_bias, head_gain, delta_state
    )
    normed = from_everyone(normed, "y").reshape(rows, -1)
    projected = times_transposed(normed, out_rows).astype(bf16)
    after_mixer = (after_first.astype(f32) + everyone_sum(projected, TP)).astype(bf16)

    hidden = hidden_units(after_mixer, jnp.dot(after_mixer, second_in, preferred_element_type=f32))
    projected = times_transposed(down_second, hidden).astype(bf16)
    pieces = jnp.concatenate([projected, after_mixer.T], axis=1)
    arrived = exchange(pieces.reshape(-1, own_cols, 2 * rows), ACROSS)
    arrived = arrived.reshape(planes, tp_count, own_cols, 2 * rows).astype(f32)
    final = arrived[:, 0, :, rows:] + 0.5 * arrived[..., :rows].sum(axis=1)
    residual_out = jnp.moveaxis(final, 1, 2).reshape(planes * rows, own_cols).astype(bf16)
    return (residual_out, new_state)


def solution(mesh):
    cut = Mesh(mesh.devices.reshape(8, 4, 4, 2), ("z", "y", "x", "c"))
    kv, tp = ("z", "y"), ("x", "c")
    wide, tall = P(kv, tp), P(tp, kv)
    placed = (
        P(None, kv + tp),
        P(kv, tp, None, None),
        P(kv),
        wide,
        wide,
        tall,
        P(kv),
        wide,
        wide,
        wide,
        wide,
        P(kv, None),
        P(kv, None),
        P(tp),
        P(tp),
        P(),
        tall,
        P(kv),
        wide,
        wide,
        tall,
    )
    return jax.shard_map(
        body,
        mesh=cut,
        in_specs=placed,
        out_specs=(P(None, kv + tp), P(kv, tp, None, None)),
        check_vma=False,
    )
```

```python
import jax
import jax.numpy as jnp
from jax import lax
from jax.sharding import Mesh
from jax.sharding import PartitionSpec as P


D = 2048
HEAD = 128
GATES = 128

epsilon = 1e-06

TP = ("x", "c")
ACROSS = ("z", "x", "c")

bf16 = jnp.bfloat16
f32 = jnp.float32


def exchange(blocks, axis):
    return lax.all_to_all(blocks, axis, split_axis=0, concat_axis=0, tiled=True)


def from_everyone(value, axis):
    return exchange(jnp.broadcast_to(value, (lax.axis_size(axis), *value.shape)), axis)


def everyone_sum(value, axis):
    return from_everyone(value, axis).astype(f32).sum(axis=0)


def ring_sum(value, axis):
    size = lax.axis_size(axis)
    total = value.astype(f32)
    for places in range(1, size):
        total = total + lax.ppermute(value, axis, [(i, (i + places) % size) for i in range(size)]).astype(f32)
    return total


def times_transposed(left, right_rows):
    return lax.dot_general(left, right_rows, (((1,), (1,)), ((), ())), preferred_element_type=f32)


def square_columns(as_float):
    squares = jnp.sum(as_float * as_float, axis=1, keepdims=True)
    high = squares.astype(bf16).astype(f32)
    lane = lax.broadcasted_iota(jnp.int32, (squares.shape[0], GATES), 1)
    return jnp.where(lane == 0, high, jnp.where(lane == 1, squares - high, 0.0))


def row_scale(first_two):
    return lax.rsqrt((first_two[:, :1] + first_two[:, 1:2]) / D + epsilon)


def around(block, axis):
    size = lax.axis_size(axis)
    ahead = [(i, (i + 1) % size) for i in range(size)]
    behind = [(i, (i - 1) % size) for i in range(size)]
    blocks = [block] + [None] * (size - 1)
    forward = backward = block
    for step in range(1, size // 2):
        forward = blocks[size - step] = lax.ppermute(forward, axis, ahead)
        backward = blocks[step] = lax.ppermute(backward, axis, behind)
    half = block.shape[1] // 2
    forward = lax.ppermute(forward[:, :half], axis, ahead)
    backward = lax.ppermute(backward[:, half:], axis, behind)
    blocks[size // 2] = jnp.concatenate([forward, backward], axis=1)
    return blocks


def hidden_units(residual, partial_value):
    both = jnp.concatenate([partial_value, square_columns(residual.astype(f32))], axis=1).astype(bf16)
    summed = ring_sum(both, "y")
    width = partial_value.shape[1]
    scale = row_scale(summed[:, width:])
    gate_act = summed[:, : width // 2] * scale
    up_act = summed[:, width // 2 : width] * scale
    return (jax.nn.silu(gate_act) * up_act).astype(bf16)


def unit_heads(projected, head_size):
    activated = jax.nn.silu(projected).reshape(projected.shape[0], -1, head_size)
    return activated * lax.rsqrt(jnp.sum(activated * activated, axis=-1, keepdims=True) + epsilon)


def delta_step(old_state, key_rows, queries, values, beta_gate, decay_gate):
    faded_state = old_state * decay_gate[:, :, None, None]
    predicted = jnp.einsum("rhab,rha->rhb", faded_state, key_rows, precision=lax.Precision.HIGHEST)
    correction = beta_gate[:, :, None] * (values - predicted)
    updated = faded_state + key_rows[:, :, :, None] * correction[:, :, None, :]
    reading = jnp.einsum("rhab,rha->rhb", updated, queries, precision=lax.Precision.HIGHEST)
    return (updated, reading)


def mixer_values(residual, mixer_in, decay_rate, decay_bias, head_gain, old_state):
    row_count, heads_dev, head_size = old_state.shape[:3]
    projected = jnp.dot(residual, mixer_in, preferred_element_type=f32)
    width = mixer_in.shape[1] - GATES
    squares = square_columns(residual.astype(f32))
    tail = projected[:, width:] + jnp.roll(squares, 2 * heads_dev, axis=1)
    both = jnp.concatenate([projected[:, :width], tail], axis=1).astype(bf16)
    blocks = both.reshape(-1, row_count, both.shape[1])
    summed = exchange(blocks, "y").astype(f32).sum(axis=0)
    tail = summed[:, width:]
    scale = row_scale(tail[:, 2 * heads_dev :])
    summed = summed[:, :width] * scale
    gates = tail * scale
    value_cols = heads_dev * head_size
    key_cols = (width - 2 * value_cols) // 2
    repeat_count = value_cols // key_cols
    queries = jnp.repeat(
        unit_heads(summed[:, :key_cols], head_size) * head_size ** (-0.5), repeat_count, axis=1
    )
    key_rows = jnp.repeat(unit_heads(summed[:, key_cols : 2 * key_cols], head_size), repeat_count, axis=1)
    values = jax.nn.silu(summed[:, 2 * key_cols : 2 * key_cols + value_cols]).reshape(
        row_count, heads_dev, head_size
    )
    out_gate = jax.nn.silu(summed[:, 2 * key_cols + value_cols :]).reshape(row_count, heads_dev, head_size)
    beta_gate = jax.nn.sigmoid(gates[:, :heads_dev])
    decay_gate = jnp.exp(
        -jnp.exp(decay_rate)[None, :]
        * jax.nn.softplus(gates[:, heads_dev : 2 * heads_dev] + decay_bias[None, :])
    )
    new_state, reading = delta_step(old_state, key_rows, queries, values, beta_gate, decay_gate)
    normed = reading * lax.rsqrt(jnp.mean(reading * reading, axis=-1, keepdims=True) + epsilon)
    normed = (normed * head_gain * out_gate).reshape(row_count, value_cols).astype(bf16)
    return normed, new_state


def body(
    residual_in,
    delta_state,
    norm_gain_first,
    gate_first,
    up_first,
    down_first,
    norm_gain_mixer,
    query_weight,
    key_weight,
    value_weight,
    output_gate_weight,
    beta_weight,
    decay_weight,
    decay_rate,
    decay_bias,
    head_gain,
    out_weight,
    norm_gain_second,
    gate_second,
    up_second,
    down_second,
):
    planes, tp_count = lax.axis_size("z"), lax.axis_size(TP)
    heads_dev = decay_rate.shape[0]

    def scaled_rows(gain, weights):
        return (jnp.concatenate(weights, axis=1).astype(f32) * gain[:, None]).astype(bf16)

    def gathered(weights):
        return lax.all_gather(jnp.concatenate(weights, axis=1), "z", axis=0, tiled=True)

    head_start = lax.axis_index(TP) * heads_dev
    gate_cols = [
        lax.dynamic_slice_in_dim(beta_weight, head_start, heads_dev, 1),
        lax.dynamic_slice_in_dim(decay_weight, head_start, heads_dev, 1),
        jnp.zeros((beta_weight.shape[0], GATES - 2 * heads_dev), bf16),
    ]
    first_in = scaled_rows(norm_gain_first, [gate_first, up_first])
    first_in, query_weight, gate_cols[0], gate_cols[1], down_first = lax.optimization_barrier(
        (first_in, query_weight, gate_cols[0], gate_cols[1], down_first)
    )
    mixer_in = scaled_rows(
        norm_gain_mixer, [query_weight, key_weight, value_weight, output_gate_weight, *gate_cols]
    )
    first_blocks = around(first_in, "z")
    first_blocks[1], first_blocks[-1], norm_gain_second, out_weight = lax.optimization_barrier(
        (first_blocks[1], first_blocks[-1], norm_gain_second, out_weight)
    )
    second_in = scaled_rows(norm_gain_second, [gate_second, up_second])
    width, mixer_width = first_in.shape[1], mixer_in.shape[1]
    middle = jnp.concatenate([mixer_in, down_first.T], axis=1)
    middle, residual_in = lax.optimization_barrier((middle, residual_in))
    middle = gathered([middle])
    mixer_in, down_first = middle[:, :mixer_width], middle[:, mixer_width:]
    last = gathered([out_weight.T, second_in, down_second.T])
    values_width = out_weight.shape[0]
    out_rows, second_in, down_second = (
        last[:, :values_width],
        last[:, values_width : values_width + width],
        last[:, values_width + width :],
    )

    columns = residual_in.T
    own_cols, rows = columns.shape[0], columns.shape[1] // planes
    pieces = jnp.moveaxis(columns.reshape(own_cols, planes, rows), 1, 0)
    pieces = jnp.broadcast_to(pieces[:, None], (planes, tp_count, own_cols, rows))
    arrived = exchange(pieces.reshape(-1, own_cols, rows), ACROSS).reshape(planes, -1, rows)
    arrived, first_blocks[2], first_blocks[-2] = lax.optimization_barrier(
        (arrived, first_blocks[2], first_blocks[-2])
    )
    residual = arrived.reshape(-1, rows).T
    twice = jnp.concatenate([arrived, arrived], axis=0)
    ahead = lax.dynamic_slice_in_dim(twice, lax.axis_index("z"), planes, 0)
    products = [
        lax.dot_general(ahead[o], first_blocks[o], (((0,), (0,)), ((), ())), preferred_element_type=f32)
        for step in range(planes // 2 + 1)
        for o in sorted({step, (planes - step) % planes})
    ]
    partial_value = products[0]
    for product in products[1:]:
        partial_value = partial_value + product

    hidden = hidden_units(residual, partial_value)
    projected = times_transposed(hidden, down_first).astype(bf16)
    after_first = (residual.astype(f32) + 0.5 * everyone_sum(projected, TP)).astype(bf16)

    normed, new_state = mixer_values(
        after_first, mixer_in, decay_rate, decay_bias, head_gain, delta_state
    )
    normed = from_everyone(normed, "y").reshape(rows, -1)
    projected = times_transposed(normed, out_rows).astype(bf16)
    after_mixer = (after_first.astype(f32) + everyone_sum(projected, TP)).astype(bf16)

    hidden = hidden_units(after_mixer, jnp.dot(after_mixer, second_in, preferred_element_type=f32))
    projected = times_transposed(down_second, hidden).astype(bf16)
    pieces = jnp.concatenate([projected, after_mixer.T], axis=1)
    arrived = exchange(pieces.reshape(-1, own_cols, 2 * rows), ACROSS)
    arrived = arrived.reshape(planes, tp_count, own_cols, 2 * rows).astype(f32)
    final = arrived[:, 0, :, rows:] + 0.5 * arrived[..., :rows].sum(axis=1)
    residual_out = jnp.moveaxis(final, 1, 2).reshape(planes * rows, own_cols).astype(bf16)
    return (residual_out, new_state)


def solution(mesh):
    cut = Mesh(mesh.devices.reshape(8, 4, 4, 2), ("z", "y", "x", "c"))
    kv, tp = ("z", "y"), ("x", "c")
    wide, tall = P(kv, tp), P(tp, kv)
    placed = (
        P(None, kv + tp),
        P(kv, tp, None, None),
        P(kv),
        wide,
        wide,
        tall,
        P(kv),
        wide,
        wide,
        wide,
        wide,
        P(kv, None),
        P(kv, None),
        P(tp),
        P(tp),
        P(),
        tall,
        P(kv),
        wide,
        wide,
        tall,
    )
    return jax.shard_map(
        body,
        mesh=cut,
        in_specs=placed,
        out_specs=(P(None, kv + tp), P(kv, tp, None, None)),
        check_vma=False,
    )
```

```python
import jax
import jax.numpy as jnp
from jax import lax
from jax.experimental import pallas as pl
from jax.experimental.pallas import tpu as pltpu
from jax.sharding import Mesh
from jax.sharding import PartitionSpec as P


D = 2048
HEAD = 128
GATES = 128

epsilon = 1e-06

TP = ("x", "c")
ACROSS = ("z", "x", "c")

bf16 = jnp.bfloat16
f32 = jnp.float32


def exchange(blocks, axis):
    return lax.all_to_all(blocks, axis, split_axis=0, concat_axis=0, tiled=True)


def from_everyone(value, axis):
    return exchange(jnp.broadcast_to(value, (lax.axis_size(axis), *value.shape)), axis)


def everyone_sum(value, axis):
    return from_everyone(value, axis).astype(f32).sum(axis=0)


def ring_sum(value, axis):
    size = lax.axis_size(axis)
    total = value.astype(f32)
    for places in range(1, size):
        total = total + lax.ppermute(value, axis, [(i, (i + places) % size) for i in range(size)]).astype(f32)
    return total


def times_transposed(left, right_rows):
    return lax.dot_general(left, right_rows, (((1,), (1,)), ((), ())), preferred_element_type=f32)


def square_columns(as_float):
    squares = jnp.sum(as_float * as_float, axis=1, keepdims=True)
    high = squares.astype(bf16).astype(f32)
    lane = lax.broadcasted_iota(jnp.int32, (squares.shape[0], GATES), 1)
    return jnp.where(lane == 0, high, jnp.where(lane == 1, squares - high, 0.0))


def row_scale(first_two):
    return lax.rsqrt((first_two[:, :1] + first_two[:, 1:2]) / D + epsilon)


def around(block, axis):
    size = lax.axis_size(axis)
    ahead = [(i, (i + 1) % size) for i in range(size)]
    behind = [(i, (i - 1) % size) for i in range(size)]
    blocks = [block] + [None] * (size - 1)
    forward = backward = block
    for step in range(1, size // 2):
        forward = blocks[size - step] = lax.ppermute(forward, axis, ahead)
        backward = blocks[step] = lax.ppermute(backward, axis, behind)
    half = block.shape[1] // 2
    forward = lax.ppermute(forward[:, :half], axis, ahead)
    backward = lax.ppermute(backward[:, half:], axis, behind)
    blocks[size // 2] = jnp.concatenate([forward, backward], axis=1)
    return blocks


def hidden_units(residual, partial_value):
    both = jnp.concatenate([partial_value, square_columns(residual.astype(f32))], axis=1).astype(bf16)
    summed = ring_sum(both, "y")
    width = partial_value.shape[1]
    scale = row_scale(summed[:, width:])
    gate_act = summed[:, : width // 2] * scale
    up_act = summed[:, width // 2 : width] * scale
    return (jax.nn.silu(gate_act) * up_act).astype(bf16)


def unit_heads(activated):
    squares = jnp.sum(activated * activated, axis=-1, keepdims=True)
    return activated * lax.rsqrt(squares + epsilon)


def mixer_kernel(
    arrived_ref, rate_ref, bias_ref, gain_ref, state_ref, out_ref, new_ref, made, read_ref, went
):
    count, heads = state_ref.shape[:2]
    pairs = heads // 2
    store = [pltpu.make_async_copy(made.at[s], new_ref.at[s], went.at[s]) for s in range(count)]
    summed = arrived_ref[0].astype(f32)
    for i in range(1, arrived_ref.shape[0]):
        summed = summed + arrived_ref[i].astype(f32)
    width = summed.shape[1] - GATES
    tail = summed[:, width:]
    scale = row_scale(tail[:, 2 * heads : 2 * heads + 2])
    gates = tail * scale
    activated = jax.nn.silu(summed[:, :width] * scale)
    beta = jax.nn.sigmoid(gates[:, :heads])
    drive = gates[:, heads : 2 * heads] + bias_ref[...]
    softplus = jnp.maximum(drive, 0.0) + jnp.log1p(jnp.exp(-jnp.abs(drive)))
    decay = jnp.exp(-jnp.exp(rate_ref[...]) * softplus)
    head = lambda at: activated[:, at * HEAD : (at + 1) * HEAD]
    rows = [unit_heads(head(m)) * HEAD ** (-0.5) for m in range(pairs)]
    rows += [unit_heads(head(pairs + m)) for m in range(pairs)]
    rows.append(jnp.zeros((HEAD - 2 * pairs * count, HEAD), f32))
    turned = jnp.concatenate(rows, axis=0).T
    for s in range(count):
        for m in range(pairs):
            at = m * count + s
            query = jnp.broadcast_to(turned[:, at : at + 1], (HEAD, HEAD))
            at += pairs * count
            key = jnp.broadcast_to(turned[:, at : at + 1], (HEAD, HEAD))
            for h in (2 * m, 2 * m + 1):
                faded = state_ref[s, h] * decay[s : s + 1, h : h + 1]
                predicted = jnp.sum(faded * key, axis=0, keepdims=True)
                value = head(2 * pairs + h)[s : s + 1]
                correction = beta[s : s + 1, h : h + 1] * (value - predicted)
                updated = faded + key * correction
                made[s, h] = updated
                read_ref[s : s + 1, h * HEAD : (h + 1) * HEAD] = jnp.sum(
                    updated * query, axis=0, keepdims=True
                )
        store[s].start()
    for h in range(heads):
        columns = slice(h * HEAD, (h + 1) * HEAD)
        reading = read_ref[:, columns]
        mean = jnp.sum(reading * reading, axis=-1, keepdims=True) / HEAD
        normed = reading * lax.rsqrt(mean + epsilon) * gain_ref[...] * head(2 * pairs + heads + h)
        for i in range(out_ref.shape[0]):
            out_ref[i, :, columns] = normed.astype(bf16)
    for copy in store:
        copy.wait()


def mixer_values(residual, mixer_in, decay_rate, decay_bias, head_gain, old_state):
    row_count, heads_dev, head_size = old_state.shape[:3]
    projected = jnp.dot(residual, mixer_in, preferred_element_type=f32)
    width = mixer_in.shape[1] - GATES
    squares = square_columns(residual.astype(f32))
    tail = projected[:, width:] + jnp.roll(squares, 2 * heads_dev, axis=1)
    both = jnp.concatenate([projected[:, :width], tail], axis=1).astype(bf16)
    arrived = exchange(both.reshape(-1, row_count, both.shape[1]), "y")
    whole = pl.BlockSpec(memory_space=pltpu.VMEM)
    return pl.pallas_call(
        mixer_kernel,
        out_shape=(
            jax.ShapeDtypeStruct((arrived.shape[0], row_count, heads_dev * head_size), bf16),
            jax.ShapeDtypeStruct(old_state.shape, f32),
        ),
        in_specs=[whole] * 5,
        out_specs=(whole, pl.BlockSpec(memory_space=pl.ANY)),
        scratch_shapes=[
            pltpu.VMEM(old_state.shape, f32),
            pltpu.VMEM((row_count, heads_dev * head_size), f32),
            pltpu.SemaphoreType.DMA((row_count,)),
        ],
        compiler_params=pltpu.CompilerParams(vmem_limit_bytes=16 * 1024 * 1024),
        cost_estimate=pl.CostEstimate(flops=20_000_000, bytes_accessed=4_200_000, transcendentals=20_000),
    )(arrived, decay_rate[None, :], decay_bias[None, :], head_gain[None, :], old_state)


def body(
    residual_in,
    delta_state,
    norm_gain_first,
    gate_first,
    up_first,
    down_first,
    norm_gain_mixer,
    query_weight,
    key_weight,
    value_weight,
    output_gate_weight,
    beta_weight,
    decay_weight,
    decay_rate,
    decay_bias,
    head_gain,
    out_weight,
    norm_gain_second,
    gate_second,
    up_second,
    down_second,
):
    planes, tp_count = lax.axis_size("z"), lax.axis_size(TP)
    heads_dev = decay_rate.shape[0]

    def scaled_rows(gain, weights):
        return (jnp.concatenate(weights, axis=1).astype(f32) * gain[:, None]).astype(bf16)

    def gathered(weights):
        return lax.all_gather(jnp.concatenate(weights, axis=1), "z", axis=0, tiled=True)

    head_start = lax.axis_index(TP) * heads_dev
    gate_cols = [
        lax.dynamic_slice_in_dim(beta_weight, head_start, heads_dev, 1),
        lax.dynamic_slice_in_dim(decay_weight, head_start, heads_dev, 1),
        jnp.zeros((beta_weight.shape[0], GATES - 2 * heads_dev), bf16),
    ]
    first_in = scaled_rows(norm_gain_first, [gate_first, up_first])
    first_in, query_weight, gate_cols[0], gate_cols[1], down_first = lax.optimization_barrier(
        (first_in, query_weight, gate_cols[0], gate_cols[1], down_first)
    )
    mixer_in = scaled_rows(
        norm_gain_mixer, [query_weight, key_weight, value_weight, output_gate_weight, *gate_cols]
    )
    first_blocks = around(first_in, "z")
    first_blocks[1], first_blocks[-1], norm_gain_second, out_weight = lax.optimization_barrier(
        (first_blocks[1], first_blocks[-1], norm_gain_second, out_weight)
    )
    second_in = scaled_rows(norm_gain_second, [gate_second, up_second])
    width, mixer_width = first_in.shape[1], mixer_in.shape[1]
    middle = jnp.concatenate([mixer_in, down_first.T], axis=1)
    middle = gathered([middle])
    mixer_in, down_first = middle[:, :mixer_width], middle[:, mixer_width:]
    last = gathered([out_weight.T, second_in, down_second.T])
    values_width = out_weight.shape[0]
    out_rows, second_in, down_second = (
        last[:, :values_width],
        last[:, values_width : values_width + width],
        last[:, values_width + width :],
    )

    columns = residual_in.T
    own_cols, rows = columns.shape[0], columns.shape[1] // planes
    pieces = jnp.moveaxis(columns.reshape(own_cols, planes, rows), 1, 0)
    pieces = jnp.broadcast_to(pieces[:, None], (planes, tp_count, own_cols, rows))
    arrived = exchange(pieces.reshape(-1, own_cols, rows), ACROSS)
    arrived = arrived.reshape(planes, -1, rows)
    arrived, first_blocks[2], first_blocks[-2] = lax.optimization_barrier(
        (arrived, first_blocks[2], first_blocks[-2])
    )
    residual = arrived.reshape(-1, rows).T
    twice = jnp.concatenate([arrived, arrived], axis=0)
    ahead = lax.dynamic_slice_in_dim(twice, lax.axis_index("z"), planes, 0)
    products = [
        lax.dot_general(ahead[o], first_blocks[o], (((0,), (0,)), ((), ())), preferred_element_type=f32)
        for step in range(planes // 2 + 1)
        for o in sorted({step, (planes - step) % planes})
    ]
    partial_value = products[0]
    for product in products[1:]:
        partial_value = partial_value + product

    hidden = hidden_units(residual, partial_value)
    projected = times_transposed(hidden, down_first).astype(bf16)
    after_first = (residual.astype(f32) + 0.5 * everyone_sum(projected, TP)).astype(bf16)

    normed, new_state = mixer_values(
        after_first, mixer_in, decay_rate, decay_bias, head_gain, delta_state
    )
    normed = exchange(normed, "y").reshape(rows, -1)
    projected = times_transposed(normed, out_rows).astype(bf16)
    after_mixer = (after_first.astype(f32) + everyone_sum(projected, TP)).astype(bf16)

    hidden = hidden_units(after_mixer, jnp.dot(after_mixer, second_in, preferred_element_type=f32))
    projected = times_transposed(down_second, hidden).astype(bf16)
    pieces = jnp.concatenate([projected, after_mixer.T], axis=1)
    arrived = exchange(pieces.reshape(-1, own_cols, 2 * rows), ACROSS)
    arrived = arrived.reshape(planes, tp_count, own_cols, 2 * rows).astype(f32)
    final = arrived[:, 0, :, rows:] + 0.5 * arrived[..., :rows].sum(axis=1)
    residual_out = jnp.moveaxis(final, 1, 2).reshape(planes * rows, own_cols).astype(bf16)
    return (residual_out, new_state)


def solution(mesh):
    cut = Mesh(mesh.devices.reshape(8, 4, 4, 2), ("z", "y", "x", "c"))
    kv, tp = ("z", "y"), ("x", "c")
    wide, tall = P(kv, tp), P(tp, kv)
    placed = (
        P(None, kv + tp),
        P(kv, tp, None, None),
        P(kv),
        wide,
        wide,
        tall,
        P(kv),
        wide,
        wide,
        wide,
        wide,
        P(kv, None),
        P(kv, None),
        P(tp),
        P(tp),
        P(),
        tall,
        P(kv),
        wide,
        wide,
        tall,
    )

    return jax.shard_map(
        body,
        mesh=cut,
        in_specs=placed,
        out_specs=(P(None, kv + tp), P(kv, tp, None, None)),
        check_vma=False,
    )
```

```python
import jax
import jax.numpy as jnp
from jax import lax
from jax.experimental import pallas as pl
from jax.experimental.pallas import tpu as pltpu
from jax.sharding import Mesh
from jax.sharding import PartitionSpec as P


D = 2048
HEAD = 128
GATES = 128

epsilon = 1e-06

TP = ("x", "c")
ACROSS = ("z", "x", "c")

bf16 = jnp.bfloat16
f32 = jnp.float32


def exchange(blocks, axis):
    return lax.all_to_all(blocks, axis, split_axis=0, concat_axis=0, tiled=True)


def from_everyone(value, axis):
    return exchange(jnp.broadcast_to(value, (lax.axis_size(axis), *value.shape)), axis)


def everyone_sum(value, axis):
    return from_everyone(value, axis).astype(f32).sum(axis=0)


def ring_sum(value, axis):
    size = lax.axis_size(axis)
    total = value.astype(f32)
    for places in range(1, size):
        total = total + lax.ppermute(value, axis, [(i, (i + places) % size) for i in range(size)]).astype(f32)
    return total


def times_transposed(left, right_rows):
    return lax.dot_general(left, right_rows, (((1,), (1,)), ((), ())), preferred_element_type=f32)


def square_columns(as_float):
    squares = jnp.sum(as_float * as_float, axis=1, keepdims=True)
    high = squares.astype(bf16).astype(f32)
    lane = lax.broadcasted_iota(jnp.int32, (squares.shape[0], GATES), 1)
    return jnp.where(lane == 0, high, jnp.where(lane == 1, squares - high, 0.0))


def row_scale(first_two):
    return lax.rsqrt((first_two[:, :1] + first_two[:, 1:2]) / D + epsilon)


def around(block, axis):
    size = lax.axis_size(axis)
    ahead = [(i, (i + 1) % size) for i in range(size)]
    behind = [(i, (i - 1) % size) for i in range(size)]
    blocks = [block] + [None] * (size - 1)
    forward = backward = block
    for step in range(1, size // 2):
        forward = blocks[size - step] = lax.ppermute(forward, axis, ahead)
        backward = blocks[step] = lax.ppermute(backward, axis, behind)
    half = block.shape[1] // 256 * 128
    forward = lax.ppermute(forward[:, :half], axis, ahead)
    backward = lax.ppermute(backward[:, half:], axis, behind)
    blocks[size // 2] = jnp.concatenate([forward, backward], axis=1)
    return blocks


def hidden_units(residual, partial_value):
    both = jnp.concatenate([partial_value, square_columns(residual.astype(f32))], axis=1).astype(bf16)
    summed = ring_sum(both, "y")
    width = partial_value.shape[1]
    scale = row_scale(summed[:, width:])
    gate_act = summed[:, : width // 2] * scale
    up_act = summed[:, width // 2 : width] * scale
    return (jax.nn.silu(gate_act) * up_act).astype(bf16)


def unit_heads(activated):
    squares = jnp.sum(activated * activated, axis=-1, keepdims=True)
    return activated * lax.rsqrt(squares + epsilon)


def mixer_kernel(
    arrived_ref, rate_ref, bias_ref, gain_ref, state_ref, out_ref, new_ref, made, read_ref, went
):
    count, heads = state_ref.shape[:2]
    pairs = heads // 2
    store = [pltpu.make_async_copy(made.at[s], new_ref.at[s], went.at[s]) for s in range(count)]
    summed = arrived_ref[0].astype(f32)
    for i in range(1, arrived_ref.shape[0]):
        summed = summed + arrived_ref[i].astype(f32)
    width = summed.shape[1] - GATES
    tail = summed[:, width:]
    scale = row_scale(tail[:, 2 * heads : 2 * heads + 2])
    gates = tail * scale
    activated = jax.nn.silu(summed[:, :width] * scale)
    beta = jax.nn.sigmoid(gates[:, :heads])
    drive = gates[:, heads : 2 * heads] + bias_ref[...]
    softplus = jnp.maximum(drive, 0.0) + jnp.log1p(jnp.exp(-jnp.abs(drive)))
    decay = jnp.exp(-jnp.exp(rate_ref[...]) * softplus)
    head = lambda at: activated[:, at * HEAD : (at + 1) * HEAD]
    rows = [unit_heads(head(m)) * HEAD ** (-0.5) for m in range(pairs)]
    rows += [unit_heads(head(pairs + m)) for m in range(pairs)]
    rows.append(jnp.zeros((HEAD - 2 * pairs * count, HEAD), f32))
    turned = jnp.concatenate(rows, axis=0).T
    for s in range(count):
        for m in range(pairs):
            at = m * count + s
            query = jnp.broadcast_to(turned[:, at : at + 1], (HEAD, HEAD))
            at += pairs * count
            key = jnp.broadcast_to(turned[:, at : at + 1], (HEAD, HEAD))
            for h in (2 * m, 2 * m + 1):
                faded = state_ref[s, h] * decay[s : s + 1, h : h + 1]
                predicted = jnp.sum(faded * key, axis=0, keepdims=True)
                value = head(2 * pairs + h)[s : s + 1]
                correction = beta[s : s + 1, h : h + 1] * (value - predicted)
                updated = faded + key * correction
                made[s, h] = updated
                read_ref[s : s + 1, h * HEAD : (h + 1) * HEAD] = jnp.sum(
                    updated * query, axis=0, keepdims=True
                )
        store[s].start()
    for h in range(heads):
        columns = slice(h * HEAD, (h + 1) * HEAD)
        reading = read_ref[:, columns]
        mean = jnp.sum(reading * reading, axis=-1, keepdims=True) / HEAD
        normed = reading * lax.rsqrt(mean + epsilon) * gain_ref[...] * head(2 * pairs + heads + h)
        for i in range(out_ref.shape[0]):
            out_ref[i, :, columns] = normed.astype(bf16)
    for copy in store:
        copy.wait()


def mixer_values(residual, mixer_in, decay_rate, decay_bias, head_gain, old_state):
    row_count, heads_dev, head_size = old_state.shape[:3]
    projected = jnp.dot(residual, mixer_in, preferred_element_type=f32)
    width = mixer_in.shape[1] - GATES
    squares = square_columns(residual.astype(f32))
    tail = projected[:, width:] + jnp.roll(squares, 2 * heads_dev, axis=1)
    both = jnp.concatenate([projected[:, :width], tail], axis=1).astype(bf16)
    arrived = exchange(both.reshape(-1, row_count, both.shape[1]), "y")
    whole = pl.BlockSpec(memory_space=pltpu.VMEM)
    return pl.pallas_call(
        mixer_kernel,
        out_shape=(
            jax.ShapeDtypeStruct((arrived.shape[0], row_count, heads_dev * head_size), bf16),
            jax.ShapeDtypeStruct(old_state.shape, f32),
        ),
        in_specs=[whole] * 5,
        out_specs=(whole, pl.BlockSpec(memory_space=pl.ANY)),
        scratch_shapes=[
            pltpu.VMEM(old_state.shape, f32),
            pltpu.VMEM((row_count, heads_dev * head_size), f32),
            pltpu.SemaphoreType.DMA((row_count,)),
        ],
        compiler_params=pltpu.CompilerParams(vmem_limit_bytes=16 * 1024 * 1024),
        cost_estimate=pl.CostEstimate(flops=20_000_000, bytes_accessed=4_200_000, transcendentals=20_000),
    )(arrived, decay_rate[None, :], decay_bias[None, :], head_gain[None, :], old_state)


def body(
    residual_in,
    delta_state,
    norm_gain_first,
    gate_first,
    up_first,
    down_first,
    norm_gain_mixer,
    query_weight,
    key_weight,
    value_weight,
    output_gate_weight,
    beta_weight,
    decay_weight,
    decay_rate,
    decay_bias,
    head_gain,
    out_weight,
    norm_gain_second,
    gate_second,
    up_second,
    down_second,
):
    planes, tp_count = lax.axis_size("z"), lax.axis_size(TP)
    heads_dev = decay_rate.shape[0]

    def scaled_rows(gain, weights):
        return (jnp.concatenate(weights, axis=1).astype(f32) * gain[:, None]).astype(bf16)

    def gathered(weights):
        return lax.all_gather(jnp.concatenate(weights, axis=1), "z", axis=0, tiled=True)

    head_start = lax.axis_index(TP) * heads_dev
    gate_cols = [
        lax.dynamic_slice_in_dim(beta_weight, head_start, heads_dev, 1),
        lax.dynamic_slice_in_dim(decay_weight, head_start, heads_dev, 1),
        jnp.zeros((beta_weight.shape[0], GATES - 2 * heads_dev), bf16),
    ]
    first_in = scaled_rows(norm_gain_first, [gate_first, up_first])
    width = first_in.shape[1]
    first_blocks = around(jnp.concatenate([first_in, down_first.T], axis=1), "z")
    mixer_in = scaled_rows(
        norm_gain_mixer, [query_weight, key_weight, value_weight, output_gate_weight, *gate_cols]
    )
    second_in = scaled_rows(norm_gain_second, [gate_second, up_second])
    mixer_width = mixer_in.shape[1]
    middle = jnp.concatenate([mixer_in, out_weight.T], axis=1)
    last = jnp.concatenate([second_in, down_second.T], axis=1)
    first_blocks[2], first_blocks[-2], middle, last = lax.optimization_barrier(
        (first_blocks[2], first_blocks[-2], middle, last)
    )
    middle = gathered([middle])
    last = gathered([last])
    mixer_in, out_rows = middle[:, :mixer_width], middle[:, mixer_width:]
    second_in, down_second = last[:, :width], last[:, width:]

    columns = residual_in.T
    own_cols, rows = columns.shape[0], columns.shape[1] // planes
    pieces = jnp.moveaxis(columns.reshape(own_cols, planes, rows), 1, 0)
    pieces = jnp.broadcast_to(pieces[:, None], (planes, tp_count, own_cols, rows))
    arrived = exchange(pieces.reshape(-1, own_cols, rows), ACROSS)
    arrived = arrived.reshape(planes, -1, rows)
    arrived, first_blocks[3], first_blocks[-3] = lax.optimization_barrier(
        (arrived, first_blocks[3], first_blocks[-3])
    )
    residual = arrived.reshape(-1, rows).T
    across = planes * own_cols * tp_count
    block_size = own_cols * tp_count
    to = lax.broadcasted_iota(jnp.int32, (across, across), 1)
    at = lax.broadcasted_iota(jnp.int32, (across, across), 0)
    turned = lax.rem(to + (planes - lax.axis_index("z")) * block_size, across)
    order = (at == turned).astype(bf16)
    twice = jnp.concatenate([arrived, arrived], axis=0)
    ahead = lax.dynamic_slice_in_dim(twice, lax.axis_index("z"), planes, 0)
    products = [
        lax.dot_general(ahead[o], first_blocks[o][:, :width], (((0,), (0,)), ((), ())), preferred_element_type=f32)
        for step in range(planes // 2 + 1)
        for o in sorted({step, (planes - step) % planes})
    ]
    partial_value = products[0]
    for product in products[1:]:
        partial_value = partial_value + product

    hidden = hidden_units(residual, partial_value)
    down_first = jnp.concatenate([block[:, width:] for block in first_blocks], axis=0)
    projected = times_transposed(hidden, down_first).astype(bf16)
    projected = jnp.dot(projected, order, preferred_element_type=f32).astype(bf16)
    after_first = (residual.astype(f32) + 0.5 * everyone_sum(projected, TP)).astype(bf16)

    normed, new_state = mixer_values(
        after_first, mixer_in, decay_rate, decay_bias, head_gain, delta_state
    )
    normed = exchange(normed, "y").reshape(rows, -1)
    projected = times_transposed(normed, out_rows).astype(bf16)
    after_mixer = (after_first.astype(f32) + everyone_sum(projected, TP)).astype(bf16)

    hidden = hidden_units(after_mixer, jnp.dot(after_mixer, second_in, preferred_element_type=f32))
    projected = times_transposed(down_second, hidden).astype(bf16)
    pieces = jnp.concatenate([projected, after_mixer.T], axis=1)
    arrived = exchange(pieces.reshape(-1, own_cols, 2 * rows), ACROSS)
    arrived = arrived.reshape(planes, tp_count, own_cols, 2 * rows).astype(f32)
    final = arrived[:, 0, :, rows:] + 0.5 * arrived[..., :rows].sum(axis=1)
    residual_out = jnp.moveaxis(final, 1, 2).reshape(planes * rows, own_cols).astype(bf16)
    return (residual_out, new_state)


def solution(mesh):
    cut = Mesh(mesh.devices.reshape(8, 4, 4, 2), ("z", "y", "x", "c"))
    kv, tp = ("z", "y"), ("x", "c")
    wide, tall = P(kv, tp), P(tp, kv)
    placed = (
        P(None, kv + tp),
        P(kv, tp, None, None),
        P(kv),
        wide,
        wide,
        tall,
        P(kv),
        wide,
        wide,
        wide,
        wide,
        P(kv, None),
        P(kv, None),
        P(tp),
        P(tp),
        P(),
        tall,
        P(kv),
        wide,
        wide,
        tall,
    )

    return jax.shard_map(
        body,
        mesh=cut,
        in_specs=placed,
        out_specs=(P(None, kv + tp), P(kv, tp, None, None)),
        check_vma=False,
    )
```

```python
import jax
import jax.numpy as jnp
import numpy as np
from jax import lax
from jax.experimental import pallas as pl
from jax.experimental.pallas import tpu as pltpu
from jax.sharding import Mesh
from jax.sharding import PartitionSpec as P


D = 2048
HEAD = 128
GATES = 128

epsilon = 1e-06

TP = ("x", "c")
ACROSS = ("z", "x", "c")

bf16 = jnp.bfloat16
f32 = jnp.float32


def exchange(blocks, axis):
    return lax.all_to_all(blocks, axis, split_axis=0, concat_axis=0, tiled=True)


def from_everyone(value, axis):
    return exchange(jnp.broadcast_to(value, (lax.axis_size(axis), *value.shape)), axis)


def everyone_sum(value, axis):
    return from_everyone(value, axis).astype(f32).sum(axis=0)


def ring_sum(value, axis):
    size = lax.axis_size(axis)
    total = value.astype(f32)
    for places in range(1, size):
        total = total + lax.ppermute(value, axis, [(i, (i + places) % size) for i in range(size)]).astype(f32)
    return total


def times_transposed(left, right_rows):
    return lax.dot_general(left, right_rows, (((1,), (1,)), ((), ())), preferred_element_type=f32)


def square_columns(as_float):
    return two_terms(jnp.sum(as_float * as_float, axis=1, keepdims=True))


def two_terms(squares):
    high = squares.astype(bf16).astype(f32)
    return high * np.eye(1, GATES, 0, np.float32) + (squares - high) * np.eye(1, GATES, 1, np.float32)


def row_scale(first_two):
    return lax.rsqrt((first_two[:, :1] + first_two[:, 1:2]) / D + epsilon)


def around(block, axis):
    size = lax.axis_size(axis)
    ahead = [(i, (i + 1) % size) for i in range(size)]
    behind = [(i, (i - 1) % size) for i in range(size)]
    blocks = [block] + [None] * (size - 1)
    forward = backward = block
    for step in range(1, size // 2):
        forward = blocks[size - step] = lax.ppermute(forward, axis, ahead)
        backward = blocks[step] = lax.ppermute(backward, axis, behind)
    half = (block.shape[1] + 128) // 256 * 128
    forward = lax.ppermute(forward[:, :half], axis, ahead)
    backward = lax.ppermute(backward[:, half:], axis, behind)
    blocks[size // 2] = jnp.concatenate([forward, backward], axis=1)
    return blocks


def hidden_units(partial_value, squares):
    both = jnp.concatenate([partial_value, squares], axis=1).astype(bf16)
    summed = ring_sum(both, "y")
    width = partial_value.shape[1]
    scale = row_scale(summed[:, width:])
    gate_act = summed[:, : width // 2] * scale
    up_act = summed[:, width // 2 : width] * scale
    return (jax.nn.silu(gate_act) * up_act).astype(bf16)


def unit_heads(activated):
    squares = jnp.sum(activated * activated, axis=-1, keepdims=True)
    return activated * lax.rsqrt(squares + epsilon)


def mixer_kernel(
    arrived_ref, rate_ref, bias_ref, gain_ref, state_ref, out_ref, new_ref, made, read_ref, went
):
    count, heads = state_ref.shape[:2]
    pairs = heads // 2
    store = [pltpu.make_async_copy(made.at[s], new_ref.at[s], went.at[s]) for s in range(count)]
    summed = arrived_ref[0].astype(f32)
    for i in range(1, arrived_ref.shape[0]):
        summed = summed + arrived_ref[i].astype(f32)
    width = summed.shape[1] - GATES
    tail = summed[:, width:]
    scale = row_scale(tail[:, 2 * heads : 2 * heads + 2])
    gates = tail * scale
    activated = jax.nn.silu(summed[:, :width] * scale)
    beta = jax.nn.sigmoid(gates[:, :heads])
    drive = gates[:, heads : 2 * heads] + bias_ref[...]
    softplus = jnp.maximum(drive, 0.0) + jnp.log1p(jnp.exp(-jnp.abs(drive)))
    decay = jnp.exp(-jnp.exp(rate_ref[...]) * softplus)
    head = lambda at: activated[:, at * HEAD : (at + 1) * HEAD]
    rows = [unit_heads(head(m)) * HEAD ** (-0.5) for m in range(pairs)]
    rows += [unit_heads(head(pairs + m)) for m in range(pairs)]
    rows.append(jnp.zeros((HEAD - 2 * pairs * count, HEAD), f32))
    turned = jnp.concatenate(rows, axis=0).T
    for s in range(count):
        for m in range(pairs):
            at = m * count + s
            query = jnp.broadcast_to(turned[:, at : at + 1], (HEAD, HEAD))
            at += pairs * count
            key = jnp.broadcast_to(turned[:, at : at + 1], (HEAD, HEAD))
            for h in (2 * m, 2 * m + 1):
                faded = state_ref[s, h] * decay[s : s + 1, h : h + 1]
                predicted = jnp.sum(faded * key, axis=0, keepdims=True)
                value = head(2 * pairs + h)[s : s + 1]
                correction = beta[s : s + 1, h : h + 1] * (value - predicted)
                updated = faded + key * correction
                made[s, h] = updated
                read_ref[s : s + 1, h * HEAD : (h + 1) * HEAD] = jnp.sum(
                    updated * query, axis=0, keepdims=True
                )
        store[s].start()
    for h in range(heads):
        columns = slice(h * HEAD, (h + 1) * HEAD)
        reading = read_ref[:, columns]
        mean = jnp.sum(reading * reading, axis=-1, keepdims=True) / HEAD
        normed = reading * lax.rsqrt(mean + epsilon) * gain_ref[...] * head(2 * pairs + heads + h)
        for i in range(out_ref.shape[0]):
            out_ref[i, :, columns] = normed.astype(bf16)
    for copy in store:
        copy.wait()


def mixer_values(residual, mixer_in, decay_rate, decay_bias, head_gain, old_state):
    row_count, heads_dev, head_size = old_state.shape[:3]
    projected = jnp.dot(residual, mixer_in, preferred_element_type=f32)
    width = mixer_in.shape[1] - GATES
    squares = square_columns(residual.astype(f32))
    tail = projected[:, width:] + jnp.roll(squares, 2 * heads_dev, axis=1)
    both = jnp.concatenate([projected[:, :width], tail], axis=1).astype(bf16)
    arrived = exchange(both.reshape(-1, row_count, both.shape[1]), "y")
    whole = pl.BlockSpec(memory_space=pltpu.VMEM)
    return pl.pallas_call(
        mixer_kernel,
        out_shape=(
            jax.ShapeDtypeStruct((arrived.shape[0], row_count, heads_dev * head_size), bf16),
            jax.ShapeDtypeStruct(old_state.shape, f32),
        ),
        in_specs=[whole] * 5,
        out_specs=(whole, pl.BlockSpec(memory_space=pl.ANY)),
        scratch_shapes=[
            pltpu.VMEM(old_state.shape, f32),
            pltpu.VMEM((row_count, heads_dev * head_size), f32),
            pltpu.SemaphoreType.DMA((row_count,)),
        ],
        compiler_params=pltpu.CompilerParams(vmem_limit_bytes=16 * 1024 * 1024),
        cost_estimate=pl.CostEstimate(flops=20_000_000, bytes_accessed=4_200_000, transcendentals=20_000),
    )(arrived, decay_rate[None, :], decay_bias[None, :], head_gain[None, :], old_state)


def body(
    residual_in,
    delta_state,
    norm_gain_first,
    gate_first,
    up_first,
    down_first,
    norm_gain_mixer,
    query_weight,
    key_weight,
    value_weight,
    output_gate_weight,
    beta_weight,
    decay_weight,
    decay_rate,
    decay_bias,
    head_gain,
    out_weight,
    norm_gain_second,
    gate_second,
    up_second,
    down_second,
):
    planes, tp_count = lax.axis_size("z"), lax.axis_size(TP)
    heads_dev = decay_rate.shape[0]

    def scaled_rows(gain, weights):
        return (jnp.concatenate(weights, axis=1).astype(f32) * gain[:, None]).astype(bf16)

    def gathered(weights):
        return lax.all_gather(jnp.concatenate(weights, axis=1), "z", axis=0, tiled=True)

    head_start = lax.axis_index(TP) * heads_dev
    gate_cols = [
        lax.dynamic_slice_in_dim(beta_weight, head_start, heads_dev, 1),
        lax.dynamic_slice_in_dim(decay_weight, head_start, heads_dev, 1),
        jnp.zeros((beta_weight.shape[0], GATES - 2 * heads_dev), bf16),
    ]
    columns = from_everyone(residual_in.T, TP)
    own_cols, batch = columns.shape[1:]
    rows, block_size = batch // planes, own_cols * tp_count
    down_blocks = around(down_first.T, "z")
    mixer_in = scaled_rows(
        norm_gain_mixer, [query_weight, key_weight, value_weight, output_gate_weight, *gate_cols]
    )
    second_in = scaled_rows(norm_gain_second, [gate_second, up_second])
    mixer_width = mixer_in.shape[1]
    middle = jnp.concatenate([mixer_in, out_weight.T], axis=1)
    last = jnp.concatenate([second_in, down_second.T], axis=1)
    residual = columns.reshape(block_size, batch).T
    as_float = residual.astype(f32)
    scaled = (as_float * norm_gain_first).astype(bf16)
    first_in = jnp.concatenate([gate_first, up_first], axis=1)
    width = first_in.shape[1]
    partial_value = jnp.dot(scaled, first_in, preferred_element_type=f32).astype(bf16)
    spare = square_columns(as_float)[:, : GATES - block_size].astype(bf16)
    pieces = jnp.concatenate([partial_value, spare, residual], axis=1)
    arrived = exchange(pieces.reshape(planes, rows, -1), "z")
    middle = gathered([middle])
    down_blocks[3], down_blocks[-3], last, plane = lax.optimization_barrier(
        (down_blocks[3], down_blocks[-3], last, lax.axis_index("z"))
    )
    last = gathered([last])
    mixer_in, out_rows = middle[:, :mixer_width], middle[:, mixer_width:]
    second_in, down_second = last[:, :width], last[:, width:]

    across = planes * block_size
    to = lax.broadcasted_iota(jnp.int32, (across, across), 1)
    at = lax.broadcasted_iota(jnp.int32, (across, across), 0)
    order = (at == lax.rem(to + (planes - plane) * block_size, across)).astype(bf16)

    residual = jnp.moveaxis(arrived[:, :, width + GATES - block_size :], 0, 1).reshape(rows, across)
    summed = arrived[:, :, : width + GATES - block_size].astype(f32).sum(axis=0)
    squares = two_terms(summed[:, width : width + 1] + summed[:, width + 1 : width + 2])
    hidden = hidden_units(summed[:, :width], squares)
    down_first = jnp.concatenate(down_blocks, axis=0)
    projected = times_transposed(hidden, down_first).astype(bf16)
    projected = jnp.dot(projected, order, preferred_element_type=f32).astype(bf16)
    after_first = (residual.astype(f32) + 0.5 * everyone_sum(projected, TP)).astype(bf16)

    normed, new_state = mixer_values(
        after_first, mixer_in, decay_rate, decay_bias, head_gain, delta_state
    )
    normed = exchange(normed, "y").reshape(rows, -1)
    projected = times_transposed(normed, out_rows).astype(bf16)
    after_mixer = (after_first.astype(f32) + everyone_sum(projected, TP)).astype(bf16)

    partial_value = jnp.dot(after_mixer, second_in, preferred_element_type=f32)
    hidden = hidden_units(partial_value, square_columns(after_mixer.astype(f32)))
    projected = times_transposed(down_second, hidden).astype(bf16)
    pieces = jnp.concatenate([projected, after_mixer.T], axis=1)
    arrived = exchange(pieces.reshape(-1, own_cols, 2 * rows), ACROSS)
    arrived = arrived.reshape(planes, tp_count, own_cols, 2 * rows).astype(f32)
    final = arrived[:, 0, :, rows:] + 0.5 * arrived[..., :rows].sum(axis=1)
    residual_out = jnp.moveaxis(final, 1, 2).reshape(planes * rows, own_cols).astype(bf16)
    return (residual_out, new_state)


def solution(mesh):
    cut = Mesh(mesh.devices.reshape(8, 4, 4, 2), ("z", "y", "x", "c"))
    kv, tp = ("z", "y"), ("x", "c")
    wide, tall = P(kv, tp), P(tp, kv)
    placed = (
        P(None, kv + tp),
        P(kv, tp, None, None),
        P(kv),
        wide,
        wide,
        tall,
        P(kv),
        wide,
        wide,
        wide,
        wide,
        P(kv, None),
        P(kv, None),
        P(tp),
        P(tp),
        P(),
        tall,
        P(kv),
        wide,
        wide,
        tall,
    )

    return jax.shard_map(
        body,
        mesh=cut,
        in_specs=placed,
        out_specs=(P(None, kv + tp), P(kv, tp, None, None)),
        check_vma=False,
    )
```

```python
import jax
import jax.numpy as jnp
import numpy as np
from jax import lax
from jax.experimental import pallas as pl
from jax.experimental.pallas import tpu as pltpu
from jax.sharding import Mesh
from jax.sharding import PartitionSpec as P


D = 2048
HEAD = 128
GATES = 128

epsilon = 1e-06

TP = ("x", "c")
ACROSS = ("z", "x", "c")

bf16 = jnp.bfloat16
f32 = jnp.float32


def exchange(blocks, axis):
    return lax.all_to_all(blocks, axis, split_axis=0, concat_axis=0, tiled=True)


def from_everyone(value, axis):
    return exchange(jnp.broadcast_to(value, (lax.axis_size(axis), *value.shape)), axis)


def everyone_sum(value, axis):
    return from_everyone(value, axis).astype(f32).sum(axis=0)


def ring_sum(value, axis):
    size = lax.axis_size(axis)
    total = value.astype(f32)
    for places in range(1, size):
        total = total + lax.ppermute(value, axis, [(i, (i + places) % size) for i in range(size)]).astype(f32)
    return total


def times_transposed(left, right_rows):
    return lax.dot_general(left, right_rows, (((1,), (1,)), ((), ())), preferred_element_type=f32)


def square_columns(as_float):
    squares = jnp.sum(as_float * as_float, axis=1, keepdims=True)
    high = squares.astype(bf16).astype(f32)
    return high * np.eye(1, GATES, 0, np.float32) + (squares - high) * np.eye(1, GATES, 1, np.float32)


def row_scale(first_two):
    return lax.rsqrt((first_two[:, :1] + first_two[:, 1:2]) / D + epsilon)


def around(block, axis):
    size = lax.axis_size(axis)
    ahead = [(i, (i + 1) % size) for i in range(size)]
    behind = [(i, (i - 1) % size) for i in range(size)]
    blocks = [block] + [None] * (size - 1)
    forward = backward = block
    for step in range(1, size // 2):
        forward = blocks[size - step] = lax.ppermute(forward, axis, ahead)
        backward = blocks[step] = lax.ppermute(backward, axis, behind)
    half = block.shape[1] // 256 * 128
    forward = lax.ppermute(forward[:, :half], axis, ahead)
    backward = lax.ppermute(backward[:, half:], axis, behind)
    blocks[size // 2] = jnp.concatenate([forward, backward], axis=1)
    return blocks


def hidden_units(residual, partial_value):
    both = jnp.concatenate([partial_value, square_columns(residual.astype(f32))], axis=1).astype(bf16)
    summed = ring_sum(both, "y")
    width = partial_value.shape[1]
    scale = row_scale(summed[:, width:])
    gate_act = summed[:, : width // 2] * scale
    up_act = summed[:, width // 2 : width] * scale
    return (jax.nn.silu(gate_act) * up_act).astype(bf16)


def unit_heads(activated):
    squares = jnp.sum(activated * activated, axis=-1, keepdims=True)
    return activated * lax.rsqrt(squares + epsilon)


def mixer_kernel(
    arrived_ref, rate_ref, bias_ref, gain_ref, state_ref, out_ref, new_ref, made, read_ref, went
):
    count, heads = state_ref.shape[:2]
    pairs = heads // 2
    store = [pltpu.make_async_copy(made.at[s], new_ref.at[s], went.at[s]) for s in range(count)]
    summed = arrived_ref[0].astype(f32)
    for i in range(1, arrived_ref.shape[0]):
        summed = summed + arrived_ref[i].astype(f32)
    width = summed.shape[1] - GATES
    tail = summed[:, width:]
    scale = row_scale(tail[:, 2 * heads : 2 * heads + 2])
    gates = tail * scale
    activated = jax.nn.silu(summed[:, :width] * scale)
    beta = jax.nn.sigmoid(gates[:, :heads])
    drive = gates[:, heads : 2 * heads] + bias_ref[...]
    softplus = jnp.maximum(drive, 0.0) + jnp.log1p(jnp.exp(-jnp.abs(drive)))
    decay = jnp.exp(-jnp.exp(rate_ref[...]) * softplus)
    head = lambda at: activated[:, at * HEAD : (at + 1) * HEAD]
    rows = [unit_heads(head(m)) * HEAD ** (-0.5) for m in range(pairs)]
    rows += [unit_heads(head(pairs + m)) for m in range(pairs)]
    rows.append(jnp.zeros((HEAD - 2 * pairs * count, HEAD), f32))
    turned = jnp.concatenate(rows, axis=0).T
    for s in range(count):
        for m in range(pairs):
            at = m * count + s
            query = jnp.broadcast_to(turned[:, at : at + 1], (HEAD, HEAD))
            at += pairs * count
            key = jnp.broadcast_to(turned[:, at : at + 1], (HEAD, HEAD))
            for h in (2 * m, 2 * m + 1):
                faded = state_ref[s, h] * decay[s : s + 1, h : h + 1]
                predicted = jnp.sum(faded * key, axis=0, keepdims=True)
                value = head(2 * pairs + h)[s : s + 1]
                correction = beta[s : s + 1, h : h + 1] * (value - predicted)
                updated = faded + key * correction
                made[s, h] = updated
                read_ref[s : s + 1, h * HEAD : (h + 1) * HEAD] = jnp.sum(
                    updated * query, axis=0, keepdims=True
                )
        store[s].start()
    for h in range(heads):
        columns = slice(h * HEAD, (h + 1) * HEAD)
        reading = read_ref[:, columns]
        mean = jnp.sum(reading * reading, axis=-1, keepdims=True) / HEAD
        normed = reading * lax.rsqrt(mean + epsilon) * gain_ref[...] * head(2 * pairs + heads + h)
        for i in range(out_ref.shape[0]):
            out_ref[i, :, columns] = normed.astype(bf16)
    for copy in store:
        copy.wait()


def mixer_values(residual, mixer_in, decay_rate, decay_bias, head_gain, old_state):
    row_count, heads_dev, head_size = old_state.shape[:3]
    projected = jnp.dot(residual, mixer_in, preferred_element_type=f32)
    width = mixer_in.shape[1] - GATES
    squares = square_columns(residual.astype(f32))
    tail = projected[:, width:] + jnp.roll(squares, 2 * heads_dev, axis=1)
    both = jnp.concatenate([projected[:, :width], tail], axis=1).astype(bf16)
    arrived = exchange(both.reshape(-1, row_count, both.shape[1]), "y")
    whole = pl.BlockSpec(memory_space=pltpu.VMEM)
    return pl.pallas_call(
        mixer_kernel,
        out_shape=(
            jax.ShapeDtypeStruct((arrived.shape[0], row_count, heads_dev * head_size), bf16),
            jax.ShapeDtypeStruct(old_state.shape, f32),
        ),
        in_specs=[whole] * 5,
        out_specs=(whole, pl.BlockSpec(memory_space=pl.ANY)),
        scratch_shapes=[
            pltpu.VMEM(old_state.shape, f32),
            pltpu.VMEM((row_count, heads_dev * head_size), f32),
            pltpu.SemaphoreType.DMA((row_count,)),
        ],
        compiler_params=pltpu.CompilerParams(vmem_limit_bytes=16 * 1024 * 1024),
        cost_estimate=pl.CostEstimate(flops=20_000_000, bytes_accessed=4_200_000, transcendentals=20_000),
    )(arrived, decay_rate[None, :], decay_bias[None, :], head_gain[None, :], old_state)


def body(
    residual_in,
    delta_state,
    norm_gain_first,
    gate_first,
    up_first,
    down_first,
    norm_gain_mixer,
    query_weight,
    key_weight,
    value_weight,
    output_gate_weight,
    beta_weight,
    decay_weight,
    decay_rate,
    decay_bias,
    head_gain,
    out_weight,
    norm_gain_second,
    gate_second,
    up_second,
    down_second,
):
    planes, tp_count = lax.axis_size("z"), lax.axis_size(TP)
    heads_dev = decay_rate.shape[0]

    def scaled_rows(gain, weights):
        return (jnp.concatenate(weights, axis=1).astype(f32) * gain[:, None]).astype(bf16)

    def gathered(weights):
        return lax.all_gather(jnp.concatenate(weights, axis=1), "z", axis=0, tiled=True)

    head_start = lax.axis_index(TP) * heads_dev
    gate_cols = [
        lax.dynamic_slice_in_dim(beta_weight, head_start, heads_dev, 1),
        lax.dynamic_slice_in_dim(decay_weight, head_start, heads_dev, 1),
        jnp.zeros((beta_weight.shape[0], GATES - 2 * heads_dev), bf16),
    ]
    first_in = scaled_rows(norm_gain_first, [gate_first, up_first])
    width = first_in.shape[1]
    first_blocks = around(jnp.concatenate([first_in, down_first.T], axis=1), "z")
    first_blocks[1], first_blocks[-1], query_weight, out_weight = lax.optimization_barrier(
        (first_blocks[1], first_blocks[-1], query_weight, out_weight)
    )
    mixer_in = scaled_rows(norm_gain_mixer, [query_weight, key_weight, value_weight, output_gate_weight, *gate_cols])
    second_in = scaled_rows(norm_gain_second, [gate_second, up_second])
    mixer_width = mixer_in.shape[1]
    middle = jnp.concatenate([mixer_in, out_weight.T], axis=1)
    last = jnp.concatenate([second_in, down_second.T], axis=1)
    columns = residual_in.T
    own_cols, rows = columns.shape[0], columns.shape[1] // planes
    pieces = jnp.moveaxis(columns.reshape(own_cols, planes, rows), 1, 0)
    pieces = jnp.broadcast_to(pieces[:, None], (planes, tp_count, own_cols, rows))
    pieces = pieces.reshape(-1, own_cols, rows)
    first_blocks[3], first_blocks[-3], last, plane = lax.optimization_barrier(
        (first_blocks[3], first_blocks[-3], last, lax.axis_index("z"))
    )
    middle = gathered([middle])
    last = gathered([last])
    mixer_in, out_rows = middle[:, :mixer_width], middle[:, mixer_width:]
    second_in, down_second = last[:, :width], last[:, width:]

    arrived = exchange(pieces, ACROSS)
    arrived = arrived.reshape(planes, -1, rows)
    arrived, first_blocks[3], first_blocks[-3] = lax.optimization_barrier(
        (arrived, first_blocks[3], first_blocks[-3])
    )
    residual = arrived.reshape(-1, rows).T
    across = planes * own_cols * tp_count
    block_size = own_cols * tp_count
    to = lax.broadcasted_iota(jnp.int32, (across, across), 1)
    at = lax.broadcasted_iota(jnp.int32, (across, across), 0)
    turned = lax.rem(to + (planes - plane) * block_size, across)
    order = (at == turned).astype(bf16)
    twice = jnp.concatenate([arrived, arrived], axis=0)
    ahead = lax.dynamic_slice_in_dim(twice, lax.axis_index("z"), planes, 0)
    products = [
        lax.dot_general(ahead[o], first_blocks[o][:, :width], (((0,), (0,)), ((), ())), preferred_element_type=f32)
        for step in range(planes // 2 + 1)
        for o in sorted({step, (planes - step) % planes})
    ]
    partial_value = products[0]
    for product in products[1:]:
        partial_value = partial_value + product

    hidden = hidden_units(residual, partial_value)
    down_first = jnp.concatenate([block[:, width:] for block in first_blocks], axis=0)
    projected = times_transposed(hidden, down_first).astype(bf16)
    projected = jnp.dot(projected, order, preferred_element_type=f32).astype(bf16)
    after_first = (residual.astype(f32) + 0.5 * everyone_sum(projected, TP)).astype(bf16)

    normed, new_state = mixer_values(
        after_first, mixer_in, decay_rate, decay_bias, head_gain, delta_state
    )
    normed = exchange(normed, "y").reshape(rows, -1)
    projected = times_transposed(normed, out_rows).astype(bf16)
    after_mixer = (after_first.astype(f32) + everyone_sum(projected, TP)).astype(bf16)

    hidden = hidden_units(after_mixer, jnp.dot(after_mixer, second_in, preferred_element_type=f32))
    projected = times_transposed(down_second, hidden).astype(bf16)
    pieces = jnp.concatenate([projected, after_mixer.T], axis=1)
    arrived = exchange(pieces.reshape(-1, own_cols, 2 * rows), ACROSS)
    arrived = arrived.reshape(planes, tp_count, own_cols, 2 * rows).astype(f32)
    final = arrived[:, 0, :, rows:] + 0.5 * arrived[..., :rows].sum(axis=1)
    residual_out = jnp.moveaxis(final, 1, 2).reshape(planes * rows, own_cols).astype(bf16)
    return (residual_out, new_state)


def solution(mesh):
    cut = Mesh(mesh.devices.reshape(8, 4, 4, 2), ("z", "y", "x", "c"))
    kv, tp = ("z", "y"), ("x", "c")
    wide, tall = P(kv, tp), P(tp, kv)
    placed = (
        P(None, kv + tp),
        P(kv, tp, None, None),
        P(kv),
        wide,
        wide,
        tall,
        P(kv),
        wide,
        wide,
        wide,
        wide,
        P(kv, None),
        P(kv, None),
        P(tp),
        P(tp),
        P(),
        tall,
        P(kv),
        wide,
        wide,
        tall,
    )

    return jax.shard_map(
        body,
        mesh=cut,
        in_specs=placed,
        out_specs=(P(None, kv + tp), P(kv, tp, None, None)),
        check_vma=False,
    )
```

```python
import jax
import jax.numpy as jnp
import numpy as np
from jax import lax
from jax.experimental import pallas as pl
from jax.experimental.pallas import tpu as pltpu
from jax.sharding import Mesh
from jax.sharding import PartitionSpec as P


D = 2048
HEAD = 128
GATES = 128
HEADS_DEV = 4

epsilon = 1e-06

TP = ("x", "c")
ACROSS = ("z", "x", "c")

bf16 = jnp.bfloat16
f32 = jnp.float32


def exchange(blocks, axis):
    return lax.all_to_all(blocks, axis, split_axis=0, concat_axis=0, tiled=True)


def from_everyone(value, axis):
    return exchange(jnp.broadcast_to(value, (lax.axis_size(axis), *value.shape)), axis)


def everyone_sum(value, axis):
    return from_everyone(value, axis).astype(f32).sum(axis=0)


def ring_sum(value, axis):
    size = lax.axis_size(axis)
    total = value.astype(f32)
    for places in range(1, size):
        total = total + lax.ppermute(value, axis, [(i, (i + places) % size) for i in range(size)]).astype(f32)
    return total


def times_transposed(left, right_rows):
    return lax.dot_general(left, right_rows, (((1,), (1,)), ((), ())), preferred_element_type=f32)


def square_columns(as_float):
    squares = jnp.sum(as_float * as_float, axis=1, keepdims=True)
    high = squares.astype(bf16).astype(f32)
    return high * np.eye(1, GATES, 0, np.float32) + (squares - high) * np.eye(1, GATES, 1, np.float32)


def row_scale(first_two):
    return lax.rsqrt((first_two[:, :1] + first_two[:, 1:2]) / D + epsilon)


def around(block, axis):
    size = lax.axis_size(axis)
    ahead = [(i, (i + 1) % size) for i in range(size)]
    behind = [(i, (i - 1) % size) for i in range(size)]
    blocks = [block] + [None] * (size - 1)
    forward = backward = block
    for step in range(1, size // 2):
        forward = blocks[size - step] = lax.ppermute(forward, axis, ahead)
        backward = blocks[step] = lax.ppermute(backward, axis, behind)
    half = block.shape[1] // 256 * 128
    forward = lax.ppermute(forward[:, :half], axis, ahead)
    backward = lax.ppermute(backward[:, half:], axis, behind)
    blocks[size // 2] = jnp.concatenate([forward, backward], axis=1)
    return blocks


def hidden_units(residual, partial_value):
    both = jnp.concatenate([partial_value, square_columns(residual.astype(f32))], axis=1).astype(bf16)
    summed = ring_sum(both, "y")
    width = partial_value.shape[1]
    scale = row_scale(summed[:, width:])
    gate_act = summed[:, : width // 2] * scale
    up_act = summed[:, width // 2 : width] * scale
    return (jax.nn.silu(gate_act) * up_act).astype(bf16)


def unit_heads(activated):
    squares = jnp.sum(activated * activated, axis=-1, keepdims=True)
    return activated * lax.rsqrt(squares + epsilon)


def mixer_kernel(
    own_ref, near_ref, far_ref, last_ref, rate_ref, bias_ref, gain_ref, state_ref, out_ref, new_ref, made, read_ref, went
):
    count, heads = state_ref.shape[:2]
    pairs = heads // 2
    store = [pltpu.make_async_copy(made.at[s], new_ref.at[s], went.at[s]) for s in range(count)]
    summed = own_ref[...].astype(f32)
    for ref in (near_ref, far_ref, last_ref):
        summed = summed + ref[...].astype(f32)
    width = summed.shape[1] - GATES
    tail = summed[:, width:]
    scale = row_scale(tail[:, 2 * heads : 2 * heads + 2])
    gates = tail * scale
    activated = jax.nn.silu(summed[:, :width] * scale)
    beta = jax.nn.sigmoid(gates[:, :heads])
    drive = gates[:, heads : 2 * heads] + bias_ref[...]
    softplus = jnp.maximum(drive, 0.0) + jnp.log1p(jnp.exp(-jnp.abs(drive)))
    decay = jnp.exp(-jnp.exp(rate_ref[...]) * softplus)
    head = lambda at: activated[:, at * HEAD : (at + 1) * HEAD]
    rows = [unit_heads(head(m)) * HEAD ** (-0.5) for m in range(pairs)]
    rows += [unit_heads(head(pairs + m)) for m in range(pairs)]
    rows.append(jnp.zeros((HEAD - 2 * pairs * count, HEAD), f32))
    turned = jnp.concatenate(rows, axis=0).T
    for s in range(count):
        for m in range(pairs):
            at = m * count + s
            query = jnp.broadcast_to(turned[:, at : at + 1], (HEAD, HEAD))
            at += pairs * count
            key = jnp.broadcast_to(turned[:, at : at + 1], (HEAD, HEAD))
            for h in (2 * m, 2 * m + 1):
                faded = state_ref[s, h] * decay[s : s + 1, h : h + 1]
                predicted = jnp.sum(faded * key, axis=0, keepdims=True)
                value = head(2 * pairs + h)[s : s + 1]
                correction = beta[s : s + 1, h : h + 1] * (value - predicted)
                updated = faded + key * correction
                made[s, h] = updated
                read_ref[s : s + 1, h * HEAD : (h + 1) * HEAD] = jnp.sum(
                    updated * query, axis=0, keepdims=True
                )
        store[s].start()
    for h in range(heads):
        columns = slice(h * HEAD, (h + 1) * HEAD)
        reading = read_ref[:, columns]
        mean = jnp.sum(reading * reading, axis=-1, keepdims=True) / HEAD
        normed = reading * lax.rsqrt(mean + epsilon) * gain_ref[...] * head(2 * pairs + heads + h)
        for i in range(out_ref.shape[0]):
            out_ref[i, :, columns] = normed.astype(bf16)
    for copy in store:
        copy.wait()


def mixer_values(residual, mixer_in, decay_rate, decay_bias, head_gain, old_state):
    row_count, heads_dev, head_size = old_state.shape[:3]
    projected = jnp.dot(residual, mixer_in, preferred_element_type=f32)
    width = mixer_in.shape[1] - GATES
    squares = square_columns(residual.astype(f32))
    tail = projected[:, width:] + jnp.roll(squares, 2 * heads_dev, axis=1)
    both = jnp.concatenate([projected[:, :width], tail], axis=1).astype(bf16)
    size = lax.axis_size("y")
    blocks = both.reshape(size, row_count, both.shape[1])
    blocks = jnp.concatenate([blocks, blocks], axis=0)
    blocks = lax.dynamic_slice_in_dim(blocks, lax.axis_index("y"), size, 0)
    parts = [blocks[0]]
    for places in range(1, size):
        parts.append(lax.ppermute(blocks[places], "y", [(i, (i + places) % size) for i in range(size)]))
    whole = pl.BlockSpec(memory_space=pltpu.VMEM)
    return pl.pallas_call(
        mixer_kernel,
        out_shape=(
            jax.ShapeDtypeStruct((size, row_count, heads_dev * head_size), bf16),
            jax.ShapeDtypeStruct(old_state.shape, f32),
        ),
        in_specs=[whole] * 8,
        out_specs=(whole, pl.BlockSpec(memory_space=pl.ANY)),
        scratch_shapes=[
            pltpu.VMEM(old_state.shape, f32),
            pltpu.VMEM((row_count, heads_dev * head_size), f32),
            pltpu.SemaphoreType.DMA((row_count,)),
        ],
        compiler_params=pltpu.CompilerParams(vmem_limit_bytes=16 * 1024 * 1024),
        cost_estimate=pl.CostEstimate(flops=20_000_000, bytes_accessed=4_200_000, transcendentals=20_000),
    )(*parts, decay_rate[None, :], decay_bias[None, :], head_gain[None, :], old_state)


def pack_kernel(
    start_ref, gains_ref, gate_ref, up_ref, down_ref, query_ref, key_ref, value_ref, out_gate_ref,
    beta_ref, decay_ref, out_ref, first_ref, middle_ref,
):
    count = gate_ref.shape[0]
    at = lambda shape, dim: lax.broadcasted_iota(jnp.int32, shape, dim)
    diagonal = at((count, count), 0) == at((count, count), 1)
    gain = lambda i: jnp.sum(jnp.where(diagonal, gains_ref[i : i + 1, :], 0.0), axis=1, keepdims=True)
    first_gain, mixer_gain = gain(0), gain(1)
    scaled = lambda ref, column: (ref[...].astype(f32) * column).astype(bf16)
    width = gate_ref.shape[1]
    first_ref[:, :width] = scaled(gate_ref, first_gain)
    first_ref[:, width : 2 * width] = scaled(up_ref, first_gain)
    first_ref[:, 2 * width :] = down_ref[...]
    place = 0
    for ref in (query_ref, key_ref, value_ref, out_gate_ref):
        middle_ref[:, place : place + ref.shape[1]] = scaled(ref, mixer_gain)
        place += ref.shape[1]
    shape = (beta_ref.shape[0], GATES)
    head, lane = at(shape, 0), at(shape, 1)
    heads = HEADS_DEV
    picked = jnp.zeros((count, GATES), f32)
    for i, ref in enumerate((beta_ref, decay_ref)):
        own = (lane >= i * heads) & (lane < (i + 1) * heads) & (head == start_ref[0] + lane - i * heads)
        picked = picked + lax.dot_general(
            ref[...], own.astype(bf16), (((0,), (0,)), ((), ())), preferred_element_type=f32
        )
    middle_ref[:, place : place + GATES] = (picked * mixer_gain).astype(bf16)
    middle_ref[:, place + GATES :] = out_ref[...]


def body(
    residual_in,
    delta_state,
    norm_gain_first,
    gate_first,
    up_first,
    down_first,
    norm_gain_mixer,
    query_weight,
    key_weight,
    value_weight,
    output_gate_weight,
    beta_weight,
    decay_weight,
    decay_rate,
    decay_bias,
    head_gain,
    out_weight,
    norm_gain_second,
    gate_second,
    up_second,
    down_second,
):
    planes, tp_count = lax.axis_size("z"), lax.axis_size(TP)
    heads_dev = decay_rate.shape[0]

    def scaled_rows(gain, weights):
        return (jnp.concatenate(weights, axis=1).astype(f32) * gain[:, None]).astype(bf16)

    def gathered(weights):
        return lax.all_gather(jnp.concatenate(weights, axis=1), "z", axis=0, tiled=True)

    width = 2 * gate_first.shape[1]
    mixer_width = 2 * query_weight.shape[1] + 2 * value_weight.shape[1] + GATES
    whole = pl.BlockSpec(memory_space=pltpu.VMEM)
    first, middle = pl.pallas_call(
        pack_kernel,
        out_shape=(
            jax.ShapeDtypeStruct((gate_first.shape[0], width + down_first.shape[0]), bf16),
            jax.ShapeDtypeStruct((gate_first.shape[0], mixer_width + out_weight.shape[0]), bf16),
        ),
        in_specs=[pl.BlockSpec(memory_space=pltpu.SMEM)] + [whole] * 11,
        out_specs=(whole, whole),
        compiler_params=pltpu.CompilerParams(vmem_limit_bytes=60 * 1024 * 1024),
        cost_estimate=pl.CostEstimate(flops=20_000_000, bytes_accessed=1_100_000, transcendentals=0),
    )(
        (lax.axis_index(TP) * heads_dev).reshape(1),
        jnp.stack([norm_gain_first, norm_gain_mixer]),
        gate_first,
        up_first,
        down_first.T,
        query_weight,
        key_weight,
        value_weight,
        output_gate_weight,
        beta_weight.T,
        decay_weight.T,
        out_weight.T,
    )
    first_blocks = around(first, "z")
    second_in = scaled_rows(norm_gain_second, [gate_second, up_second])
    last = jnp.concatenate([second_in, down_second.T], axis=1)
    columns = residual_in.T
    own_cols, rows = columns.shape[0], columns.shape[1] // planes
    pieces = jnp.moveaxis(columns.reshape(own_cols, planes, rows), 1, 0)
    pieces = jnp.broadcast_to(pieces[:, None], (planes, tp_count, own_cols, rows))
    pieces = pieces.reshape(-1, own_cols, rows)
    first_blocks[3], first_blocks[-3], last, plane = lax.optimization_barrier(
        (first_blocks[3], first_blocks[-3], last, lax.axis_index("z"))
    )
    middle = gathered([middle])
    last = gathered([last])
    mixer_in, out_rows = middle[:, :mixer_width], middle[:, mixer_width:]
    second_in, down_second = last[:, :width], last[:, width:]

    arrived = exchange(pieces, ACROSS)
    arrived = arrived.reshape(planes, -1, rows)
    arrived, first_blocks[3], first_blocks[-3] = lax.optimization_barrier(
        (arrived, first_blocks[3], first_blocks[-3])
    )
    residual = arrived.reshape(-1, rows).T
    across = planes * own_cols * tp_count
    block_size = own_cols * tp_count
    to = lax.broadcasted_iota(jnp.int32, (across, across), 1)
    at = lax.broadcasted_iota(jnp.int32, (across, across), 0)
    turned = lax.rem(to + (planes - plane) * block_size, across)
    order = (at == turned).astype(bf16)
    twice = jnp.concatenate([arrived, arrived], axis=0)
    ahead = lax.dynamic_slice_in_dim(twice, lax.axis_index("z"), planes, 0)
    products = [
        lax.dot_general(ahead[o], first_blocks[o][:, :width], (((0,), (0,)), ((), ())), preferred_element_type=f32)
        for step in range(planes // 2 + 1)
        for o in sorted({step, (planes - step) % planes})
    ]
    partial_value = products[0]
    for product in products[1:]:
        partial_value = partial_value + product

    hidden = hidden_units(residual, partial_value)
    down_first = jnp.concatenate([block[:, width:] for block in first_blocks], axis=0)
    projected = times_transposed(hidden, down_first).astype(bf16)
    projected = jnp.dot(projected, order, preferred_element_type=f32).astype(bf16)
    after_first = (residual.astype(f32) + 0.5 * everyone_sum(projected, TP)).astype(bf16)

    normed, new_state = mixer_values(
        after_first, mixer_in, decay_rate, decay_bias, head_gain, delta_state
    )
    normed = exchange(normed, "y").reshape(rows, -1)
    projected = times_transposed(normed, out_rows).astype(bf16)
    after_mixer = (after_first.astype(f32) + everyone_sum(projected, TP)).astype(bf16)

    hidden = hidden_units(after_mixer, jnp.dot(after_mixer, second_in, preferred_element_type=f32))
    projected = times_transposed(down_second, hidden).astype(bf16)
    pieces = jnp.concatenate([projected, after_mixer.T], axis=1)
    arrived = exchange(pieces.reshape(-1, own_cols, 2 * rows), ACROSS)
    arrived = arrived.reshape(planes, tp_count, own_cols, 2 * rows).astype(f32)
    final = arrived[:, 0, :, rows:] + 0.5 * arrived[..., :rows].sum(axis=1)
    residual_out = jnp.moveaxis(final, 1, 2).reshape(planes * rows, own_cols).astype(bf16)
    return (residual_out, new_state)


def solution(mesh):
    cut = Mesh(mesh.devices.reshape(8, 4, 4, 2), ("z", "y", "x", "c"))
    kv, tp = ("z", "y"), ("x", "c")
    wide, tall = P(kv, tp), P(tp, kv)
    placed = (
        P(None, kv + tp),
        P(kv, tp, None, None),
        P(kv),
        wide,
        wide,
        tall,
        P(kv),
        wide,
        wide,
        wide,
        wide,
        P(kv, None),
        P(kv, None),
        P(tp),
        P(tp),
        P(),
        tall,
        P(kv),
        wide,
        wide,
        tall,
    )

    return jax.shard_map(
        body,
        mesh=cut,
        in_specs=placed,
        out_specs=(P(None, kv + tp), P(kv, tp, None, None)),
        check_vma=False,
    )
```

```python
import jax
import jax.numpy as jnp
import numpy as np
from jax import lax
from jax.experimental import pallas as pl
from jax.experimental.pallas import tpu as pltpu
from jax.sharding import Mesh
from jax.sharding import PartitionSpec as P


D = 2048
HEAD = 128
GATES = 128

epsilon = 1e-06

TP = ("x", "c")
ACROSS = ("z", "x", "c")

bf16 = jnp.bfloat16
f32 = jnp.float32


def exchange(blocks, axis):
    return lax.all_to_all(blocks, axis, split_axis=0, concat_axis=0, tiled=True)


def from_everyone(value, axis):
    return exchange(jnp.broadcast_to(value, (lax.axis_size(axis), *value.shape)), axis)


def everyone_sum(value, axis):
    return from_everyone(value, axis).astype(f32).sum(axis=0)


def ring_sum(value, axis):
    size = lax.axis_size(axis)
    total = value.astype(f32)
    for places in range(1, size):
        total = total + lax.ppermute(value, axis, [(i, (i + places) % size) for i in range(size)]).astype(f32)
    return total


def times_transposed(left, right_rows):
    return lax.dot_general(left, right_rows, (((1,), (1,)), ((), ())), preferred_element_type=f32)


def square_columns(as_float):
    squares = jnp.sum(as_float * as_float, axis=1, keepdims=True)
    high = squares.astype(bf16).astype(f32)
    return high * np.eye(1, GATES, 0, np.float32) + (squares - high) * np.eye(1, GATES, 1, np.float32)


def row_scale(first_two):
    return lax.rsqrt((first_two[:, :1] + first_two[:, 1:2]) / D + epsilon)


def around(block, axis):
    size = lax.axis_size(axis)
    ahead = [(i, (i + 1) % size) for i in range(size)]
    behind = [(i, (i - 1) % size) for i in range(size)]
    blocks = [block] + [None] * (size - 1)
    forward = backward = block
    for step in range(1, size // 2):
        forward = blocks[size - step] = lax.ppermute(forward, axis, ahead)
        backward = blocks[step] = lax.ppermute(backward, axis, behind)
    half = block.shape[1] // 256 * 128
    forward = lax.ppermute(forward[:, :half], axis, ahead)
    backward = lax.ppermute(backward[:, half:], axis, behind)
    blocks[size // 2] = jnp.concatenate([forward, backward], axis=1)
    return blocks


def hidden_units(residual, partial_value):
    both = jnp.concatenate([partial_value, square_columns(residual.astype(f32))], axis=1).astype(bf16)
    summed = ring_sum(both, "y")
    width = partial_value.shape[1]
    scale = row_scale(summed[:, width:])
    gate_act = summed[:, : width // 2] * scale
    up_act = summed[:, width // 2 : width] * scale
    return (jax.nn.silu(gate_act) * up_act).astype(bf16)


def unit_heads(activated):
    squares = jnp.sum(activated * activated, axis=-1, keepdims=True)
    return activated * lax.rsqrt(squares + epsilon)


def mixer_kernel(
    arrived_ref, rate_ref, bias_ref, gain_ref, state_ref, out_ref, new_ref, made, read_ref, went
):
    count, heads = state_ref.shape[:2]
    pairs = heads // 2
    store = [pltpu.make_async_copy(made.at[s], new_ref.at[s], went.at[s]) for s in range(count)]
    summed = arrived_ref[0].astype(f32)
    for i in range(1, arrived_ref.shape[0]):
        summed = summed + arrived_ref[i].astype(f32)
    width = summed.shape[1] - GATES
    tail = summed[:, width:]
    scale = row_scale(tail[:, 2 * heads : 2 * heads + 2])
    gates = tail * scale
    activated = jax.nn.silu(summed[:, :width] * scale)
    beta = jax.nn.sigmoid(gates[:, :heads])
    drive = gates[:, heads : 2 * heads] + bias_ref[...]
    softplus = jnp.maximum(drive, 0.0) + jnp.log1p(jnp.exp(-jnp.abs(drive)))
    decay = jnp.exp(-jnp.exp(rate_ref[...]) * softplus)
    head = lambda at: activated[:, at * HEAD : (at + 1) * HEAD]
    rows = [unit_heads(head(m)) * HEAD ** (-0.5) for m in range(pairs)]
    rows += [unit_heads(head(pairs + m)) for m in range(pairs)]
    rows.append(jnp.zeros((HEAD - 2 * pairs * count, HEAD), f32))
    turned = jnp.concatenate(rows, axis=0).T
    for s in range(count):
        for m in range(pairs):
            at = m * count + s
            query = jnp.broadcast_to(turned[:, at : at + 1], (HEAD, HEAD))
            at += pairs * count
            key = jnp.broadcast_to(turned[:, at : at + 1], (HEAD, HEAD))
            for h in (2 * m, 2 * m + 1):
                faded = state_ref[s, h] * decay[s : s + 1, h : h + 1]
                predicted = jnp.sum(faded * key, axis=0, keepdims=True)
                value = head(2 * pairs + h)[s : s + 1]
                correction = beta[s : s + 1, h : h + 1] * (value - predicted)
                updated = faded + key * correction
                made[s, h] = updated
                read_ref[s : s + 1, h * HEAD : (h + 1) * HEAD] = jnp.sum(
                    updated * query, axis=0, keepdims=True
                )
        store[s].start()
    for h in range(heads):
        columns = slice(h * HEAD, (h + 1) * HEAD)
        reading = read_ref[:, columns]
        mean = jnp.sum(reading * reading, axis=-1, keepdims=True) / HEAD
        normed = reading * lax.rsqrt(mean + epsilon) * gain_ref[...] * head(2 * pairs + heads + h)
        for i in range(out_ref.shape[0]):
            out_ref[i, :, columns] = normed.astype(bf16)
    for copy in store:
        copy.wait()


def mixer_values(residual, mixer_in, decay_rate, decay_bias, head_gain, old_state):
    row_count, heads_dev, head_size = old_state.shape[:3]
    projected = jnp.dot(residual, mixer_in, preferred_element_type=f32)
    width = mixer_in.shape[1] - GATES
    squares = square_columns(residual.astype(f32))
    tail = projected[:, width:] + jnp.roll(squares, 2 * heads_dev, axis=1)
    both = jnp.concatenate([projected[:, :width], tail], axis=1).astype(bf16)
    arrived = exchange(both.reshape(-1, row_count, both.shape[1]), "y")
    whole = pl.BlockSpec(memory_space=pltpu.VMEM)
    return pl.pallas_call(
        mixer_kernel,
        out_shape=(
            jax.ShapeDtypeStruct((arrived.shape[0], row_count, heads_dev * head_size), bf16),
            jax.ShapeDtypeStruct(old_state.shape, f32),
        ),
        in_specs=[whole] * 5,
        out_specs=(whole, pl.BlockSpec(memory_space=pl.ANY)),
        scratch_shapes=[
            pltpu.VMEM(old_state.shape, f32),
            pltpu.VMEM((row_count, heads_dev * head_size), f32),
            pltpu.SemaphoreType.DMA((row_count,)),
        ],
        compiler_params=pltpu.CompilerParams(vmem_limit_bytes=16 * 1024 * 1024),
        cost_estimate=pl.CostEstimate(flops=20_000_000, bytes_accessed=4_200_000, transcendentals=20_000),
    )(arrived, decay_rate[None, :], decay_bias[None, :], head_gain[None, :], old_state)


def body(
    residual_in,
    delta_state,
    norm_gain_first,
    gate_first,
    up_first,
    down_first,
    norm_gain_mixer,
    query_weight,
    key_weight,
    value_weight,
    output_gate_weight,
    beta_weight,
    decay_weight,
    decay_rate,
    decay_bias,
    head_gain,
    out_weight,
    norm_gain_second,
    gate_second,
    up_second,
    down_second,
):
    planes, tp_count = lax.axis_size("z"), lax.axis_size(TP)
    heads_dev = decay_rate.shape[0]

    def scaled_rows(gain, weights):
        return (jnp.concatenate(weights, axis=1).astype(f32) * gain[:, None]).astype(bf16)

    def gathered(weights):
        return lax.all_gather(jnp.concatenate(weights, axis=1), "z", axis=0, tiled=True)

    head_start = lax.axis_index(TP) * heads_dev
    gate_cols = [
        lax.dynamic_slice_in_dim(beta_weight, head_start, heads_dev, 1),
        lax.dynamic_slice_in_dim(decay_weight, head_start, heads_dev, 1),
        jnp.zeros((beta_weight.shape[0], GATES - 2 * heads_dev), bf16),
    ]
    first_in = scaled_rows(norm_gain_first, [gate_first, up_first])
    width = first_in.shape[1]
    first_blocks = around(jnp.concatenate([first_in, down_first.T], axis=1), "z")
    mixer_in = scaled_rows(norm_gain_mixer, [query_weight, key_weight, value_weight, output_gate_weight, *gate_cols])
    second_in = scaled_rows(norm_gain_second, [gate_second, up_second])
    mixer_width = mixer_in.shape[1]
    middle = jnp.concatenate([mixer_in, out_weight.T], axis=1)
    last = jnp.concatenate([second_in, down_second.T], axis=1)
    columns = residual_in.T
    own_cols, rows = columns.shape[0], columns.shape[1] // planes
    pieces = jnp.moveaxis(columns.reshape(own_cols, planes, rows), 1, 0)
    pieces = jnp.broadcast_to(pieces[:, None], (planes, tp_count, own_cols, rows))
    pieces, middle = lax.optimization_barrier((pieces.reshape(-1, own_cols, rows), middle))
    first_blocks[1], first_blocks[-1], middle = lax.optimization_barrier(
        (first_blocks[1], first_blocks[-1], middle)
    )
    first_blocks[3], first_blocks[-3], last, plane = lax.optimization_barrier(
        (first_blocks[3], first_blocks[-3], last, lax.axis_index("z"))
    )
    middle = gathered([middle])
    last = gathered([last])
    mixer_in, out_rows = middle[:, :mixer_width], middle[:, mixer_width:]
    second_in, down_second = last[:, :width], last[:, width:]

    arrived = exchange(pieces, ACROSS)
    arrived = arrived.reshape(planes, -1, rows)
    arrived, first_blocks[3], first_blocks[-3] = lax.optimization_barrier(
        (arrived, first_blocks[3], first_blocks[-3])
    )
    residual = arrived.reshape(-1, rows).T
    across = planes * own_cols * tp_count
    block_size = own_cols * tp_count
    to = lax.broadcasted_iota(jnp.int32, (across, across), 1)
    at = lax.broadcasted_iota(jnp.int32, (across, across), 0)
    turned = lax.rem(to + (planes - plane) * block_size, across)
    order = (at == turned).astype(bf16)
    twice = jnp.concatenate([arrived, arrived], axis=0)
    ahead = lax.dynamic_slice_in_dim(twice, lax.axis_index("z"), planes, 0)
    products = [
        lax.dot_general(ahead[o], first_blocks[o][:, :width], (((0,), (0,)), ((), ())), preferred_element_type=f32)
        for step in range(planes // 2 + 1)
        for o in sorted({step, (planes - step) % planes})
    ]
    partial_value = products[0]
    for product in products[1:]:
        partial_value = partial_value + product

    hidden = hidden_units(residual, partial_value)
    down_first = jnp.concatenate([block[:, width:] for block in first_blocks], axis=0)
    projected = times_transposed(hidden, down_first).astype(bf16)
    projected = jnp.dot(projected, order, preferred_element_type=f32).astype(bf16)
    after_first = (residual.astype(f32) + 0.5 * everyone_sum(projected, TP)).astype(bf16)

    normed, new_state = mixer_values(
        after_first, mixer_in, decay_rate, decay_bias, head_gain, delta_state
    )
    normed = exchange(normed, "y").reshape(rows, -1)
    projected = times_transposed(normed, out_rows).astype(bf16)
    after_mixer = (after_first.astype(f32) + everyone_sum(projected, TP)).astype(bf16)

    hidden = hidden_units(after_mixer, jnp.dot(after_mixer, second_in, preferred_element_type=f32))
    projected = times_transposed(down_second, hidden).astype(bf16)
    pieces = jnp.concatenate([projected, after_mixer.T], axis=1)
    arrived = exchange(pieces.reshape(-1, own_cols, 2 * rows), ACROSS)
    arrived = arrived.reshape(planes, tp_count, own_cols, 2 * rows).astype(f32)
    final = arrived[:, 0, :, rows:] + 0.5 * arrived[..., :rows].sum(axis=1)
    residual_out = jnp.moveaxis(final, 1, 2).reshape(planes * rows, own_cols).astype(bf16)
    return (residual_out, new_state)


def solution(mesh):
    cut = Mesh(mesh.devices.reshape(8, 4, 4, 2), ("z", "y", "x", "c"))
    kv, tp = ("z", "y"), ("x", "c")
    wide, tall = P(kv, tp), P(tp, kv)
    placed = (
        P(None, kv + tp),
        P(kv, tp, None, None),
        P(kv),
        wide,
        wide,
        tall,
        P(kv),
        wide,
        wide,
        wide,
        wide,
        P(kv, None),
        P(kv, None),
        P(tp),
        P(tp),
        P(),
        tall,
        P(kv),
        wide,
        wide,
        tall,
    )

    return jax.shard_map(
        body,
        mesh=cut,
        in_specs=placed,
        out_specs=(P(None, kv + tp), P(kv, tp, None, None)),
        check_vma=False,
    )
```
